128 devices in a mesh: sp: 32 (over z, y, core), tp: 4 (over x).
Axes of the slice: x: 4, y: 4, z: 4, core: 2. Of those that a mesh axis runs over, the one named last changes fastest.
Arguments:
- residual: bfloat16 [12288, 2048], P('sp'), may hold values from -50 to 50
- queries_a: bfloat16 [12288, 512], P('sp', 'tp'), may hold values from -50 to 50
- keys_a: bfloat16 [12288, 512], P('sp', 'tp'), may hold values from -9 to 9
- values_a: bfloat16 [12288, 512], P('sp', 'tp'), may hold values from -6 to 6
- queries_b: bfloat16 [12288, 1024], P('sp', 'tp'), may hold values from -50 to 50
- keys_b: bfloat16 [12288, 1024], P('sp', 'tp'), may hold values from -9 to 9
- values_b: bfloat16 [12288, 512], P('sp', 'tp'), may hold values from -6 to 6
- mix_lambda: float32 [2, 4], P(None, 'tp'), may hold values from 0.3 to 0.8
- head_gain: float32 [2, 128], replicated, may hold values from 0.1 to 1.9
- out_a: bfloat16 [512, 2048], P('tp'), may hold values from -0.1875 to 0.1875
- out_b: bfloat16 [512, 2048], P('tp'), may hold values from -0.1875 to 0.1875
- norm_gain: float32 [2048], replicated, may hold values from 0.1 to 1.9
- w_gate: bfloat16 [2048, 5632], P('sp', 'tp'), may hold values from -0.125 to 0.125
- w_up: bfloat16 [2048, 5632], P('sp', 'tp'), may hold values from -0.125 to 0.125
- w_down: bfloat16 [5632, 2048], P('tp', 'sp'), may hold values from -0.21875 to 0.21875
Outputs:
- layer_out: bfloat16 [12288, 2048], P('sp', 'tp')
The draws below stay inside these ranges and needn't reach their ends.
All inputs are finite; a program needn't handle non-finite values.
Results may differ from the reference program's by a relative error of at most 0.0085.
Values may be sent and summed in bfloat16 or wider, within the bound.
No kernel may reach another device: no remote copies, remote signals or barrier semaphores. Data moves between devices by JAX's collectives and lax.ppermute only.
A program may use at most 256 MiB of HBM per device.

```python
import math
import jax
import jax.numpy as jnp
from jax import lax

D = 2048
FF = 5632
HEADS = 4
QA = 64
QB = 128
VD = 128
TOKENS = 12288


def draw_residual(key, part):
    base = jax.random.fold_in(key, 3)
    first, second = jax.random.split(base, 2)
    column = jnp.arange(D, dtype=jnp.float32) / D
    noise = jnp.clip(jax.random.normal(first, (TOKENS, D), jnp.float32), -6.0, 6.0)
    columns = 0.4 * 10.0 ** column
    row_scale = 2.0 ** jax.random.uniform(second, (TOKENS, 1), jnp.float32, -1.0, 1.0)
    return (noise * columns[None, :] * row_scale).astype(jnp.bfloat16)


def paired(key, width, salt):
    base = jax.random.fold_in(key, salt)
    query_seed, key_seed = jax.random.split(base, 2)
    columns = HEADS * 2 * width
    queries = 1.3 * jnp.clip(jax.random.normal(query_seed, (TOKENS, columns), jnp.float32), -6.0, 6.0)
    keys = 1.3 * jnp.clip(jax.random.normal(key_seed, (TOKENS, columns), jnp.float32), -6.0, 6.0)
    return (queries, keys)


def draw_queries_a(key, part):
    return paired(key, QA, 11)[0].astype(jnp.bfloat16)


def draw_keys_a(key, part):
    return paired(key, QA, 11)[1].astype(jnp.bfloat16)


def draw_queries_b(key, part):
    return paired(key, QB, 13)[0].astype(jnp.bfloat16)


def draw_keys_b(key, part):
    return paired(key, QB, 13)[1].astype(jnp.bfloat16)


def block_scale(rng, extent, pieces, least, largest):
    def one(position, blocks):
        draws = jax.random.uniform(jax.random.fold_in(jax.random.fold_in(rng, 6), position), (blocks,), jnp.float32, least / len(pieces), largest / len(pieces))
        return jnp.repeat(jnp.exp(draws), extent[position] // blocks).reshape((-1,) + (1,) * (len(extent) - position - 1))

    level = one(*pieces[0])
    for cut in pieces[1:]:
        level = level * one(*cut)
    return level


def scatter_about(key, shape, scale, limit, cuts=(), kind=jnp.bfloat16):
    level = block_scale(key, shape, cuts, -0.22, 0.18) if cuts else 1.0
    values = jax.random.normal(key, shape, jnp.float32) * scale * level
    return jnp.minimum(jnp.maximum(values, -limit), limit).astype(kind)


def setup_inputs(seed: int = 0) -> dict:
    streams_of = jax.random.split(jax.random.key(seed), 16)
    return {
        "residual": draw_residual(jax.random.fold_in(streams_of[15], 71), 0),
        "queries_a": draw_queries_a(jax.random.fold_in(streams_of[15], 71), 0),
        "keys_a": draw_keys_a(jax.random.fold_in(streams_of[15], 71), 0),
        "values_a": scatter_about(streams_of[3], (TOKENS, HEADS * VD), 1.0, 6.0, ((0, 32), (1, 4))),
        "queries_b": draw_queries_b(jax.random.fold_in(streams_of[15], 71), 0),
        "keys_b": draw_keys_b(jax.random.fold_in(streams_of[15], 71), 0),
        "values_b": scatter_about(streams_of[6], (TOKENS, HEADS * VD), 1.0, 6.0, ((0, 32), (1, 4))),
        "mix_lambda": jnp.clip(0.3 + 0.5 * jax.random.uniform(streams_of[7], (2, HEADS), jnp.float32) ** block_scale(streams_of[7], (2, HEADS), ((1, 4),), -0.2, 0.2), 0.3, 0.8),
        "head_gain": jnp.clip(1.0 + 0.18 * jax.random.normal(streams_of[8], (2, VD), jnp.float32), 0.1, 1.9),
        "out_a": scatter_about(streams_of[9], (HEADS * VD, D), (2 * HEADS * VD) ** -0.5, 0.1875, ((0, 4),)),
        "out_b": scatter_about(streams_of[10], (HEADS * VD, D), (2 * HEADS * VD) ** -0.5, 0.1875, ((0, 4),)),
        "norm_gain": jnp.clip(1.0 + 0.18 * jax.random.normal(streams_of[11], (D,), jnp.float32), 0.1, 1.9),
        "w_gate": scatter_about(streams_of[12], (D, FF), D ** -0.5, 0.125, ((0, 32), (1, 4))),
        "w_up": scatter_about(streams_of[13], (D, FF), D ** -0.5, 0.125, ((0, 32), (1, 4))),
        "w_down": scatter_about(streams_of[14], (FF, D), (FF // 8) ** -0.5, 0.21875, ((0, 4), (1, 32))),
    }


eps_norm = 1e-06
head_scale = 0.8

def group_attend(queries, keys, values, lambdas, gain, width):
    total = queries.shape[0]
    heads = lambdas.shape[0]
    block = math.gcd(total, 512)
    query_blocks = queries.reshape(total // block, block, heads, 2, width)
    key_rows = keys.reshape(total, heads, 2, width).astype(jnp.float32)
    value_rows = values.reshape(total, heads, values.shape[1] // heads).astype(jnp.float32)

    def one_block(query_block):
        scores = jnp.einsum('qhme,khme->mhqk', query_block.astype(jnp.float32), key_rows) * width ** (-0.5)
        peak = lax.optimization_barrier(jnp.max(scores, axis=-1, keepdims=True))
        weights = jnp.exp(scores - peak)
        denom = lax.optimization_barrier(jnp.sum(weights, axis=-1))
        rounded = lax.optimization_barrier(weights.astype(jnp.bfloat16)).astype(jnp.float32)
        numer = jnp.einsum('mhqk,khv->mhqv', rounded, value_rows)
        ratio = numer / denom[..., None]
        mixed = ratio[0] - lambdas[:, None, None] * ratio[1]
        inverse = lax.rsqrt(lax.optimization_barrier(jnp.mean(mixed * mixed, axis=-1, keepdims=True)) + eps_norm)
        normed = mixed * inverse * gain * head_scale
        return jnp.transpose(normed, (1, 0, 2)).reshape(block, -1).astype(jnp.bfloat16)
    return lax.map(one_block, query_blocks).reshape(total, -1)

def reference(residual, queries_a, keys_a, values_a, queries_b, keys_b, values_b, mix_lambda, head_gain, out_a, out_b, norm_gain, w_gate, w_up, w_down):
    heads_a = group_attend(queries_a, keys_a, values_a, mix_lambda[0], head_gain[0], QA)
    heads_b = group_attend(queries_b, keys_b, values_b, mix_lambda[1], head_gain[1], QB)
    total = residual.shape[0]
    block = math.gcd(total, 2048)
    count = total // block

    def row_block(inputs):
        residual_rows, first_rows, second_rows = inputs
        mixed = jnp.dot(first_rows, out_a, preferred_element_type=jnp.float32)
        mixed = mixed + jnp.dot(second_rows, out_b, preferred_element_type=jnp.float32)
        summed = residual_rows.astype(jnp.float32) + mixed
        inverse = lax.rsqrt(lax.optimization_barrier(jnp.mean(summed * summed, axis=-1, keepdims=True)) + eps_norm)
        normed = (summed * inverse * norm_gain).astype(jnp.bfloat16)
        gate = jnp.dot(normed, w_gate, preferred_element_type=jnp.float32)
        upward = jnp.dot(normed, w_up, preferred_element_type=jnp.float32)
        hidden = (jax.nn.silu(gate) * upward).astype(jnp.bfloat16)
        channel = jnp.dot(hidden, w_down, preferred_element_type=jnp.float32)
        return (summed + 0.5 * channel).astype(jnp.bfloat16)
    result = lax.map(row_block, (residual.reshape(count, block, -1), heads_a.reshape(count, block, -1), heads_b.reshape(count, block, -1)))
    return result.reshape(total, -1)
```

```python
import math
import functools
import jax
import jax.numpy as jnp
from jax import lax
from jax.experimental import pallas as pl
from jax.experimental.pallas import tpu as pltpu
from jax.sharding import PartitionSpec as P

eps_norm = 1e-06
head_scale = 0.8
log2e = math.log2(math.e)
f32 = jnp.float32
bf16 = jnp.bfloat16

SP = [(z, y, c) for z in range(4) for y in range(4) for c in range(2)]


def place(z, y, c):
    return (z % 4) * 8 + (y % 4) * 2 + c % 2


def along_y(x, k):
    return lax.ppermute(x, "sp", [(place(z, y, c), place(z, y + k, c)) for z, y, c in SP])


def along_z(x, k):
    return lax.ppermute(x, "sp", [(place(z, y, c), place(z + k, y, c)) for z, y, c in SP])


def other_core(x):
    return lax.ppermute(x, "sp", [(place(z, y, c), place(z, y, c + 1)) for z, y, c in SP])


def along_x(x, k):
    return lax.ppermute(x, "tp", [(i, (i + k) % 4) for i in range(4)])


def dot(a, b, ca, cb):
    return lax.dot_general(a, b, (((ca,), (cb,)), ((), ())), preferred_element_type=f32)


PER = 2


def attend_body(nq, nk, carry, last, consts, rows, wa, wb, vd, *refs):
    q_refs, refs = refs[:nq], refs[nq:]
    kv_refs, refs = refs[:nk], refs[nk:]
    if carry:
        acc_in, ml_in, refs = refs[0], refs[1], refs[2:]
    if last:
        o_ref, ml_ref, q_buf, kv_buf, q_sem, kv_sem, acc_ref = refs
    else:
        acc_ref, ml_ref, q_buf, kv_buf, q_sem, kv_sem = refs
    for i in range(nq):
        pltpu.make_async_copy(q_refs[i], q_buf.at[i], q_sem.at[i]).start()
    for i in range(nk):
        pltpu.make_async_copy(kv_refs[i], kv_buf.at[pl.ds(i * rows, rows)], kv_sem.at[i]).start()
    if carry:
        acc_ref[...] = acc_in[...]
        ml_ref[...] = ml_in[...]
    else:
        acc_ref[...] = jnp.zeros_like(acc_ref)
        ml_ref[:, 0:4, :] = jnp.full((nq, 4, rows), -jnp.inf, f32)
        ml_ref[:, 4:8, :] = jnp.zeros((nq, 4, rows), f32)
    for i in range(nq):
        pltpu.make_async_copy(q_refs[i], q_buf.at[i], q_sem.at[i]).wait()
    per = min(PER, nk)
    steps = nk // per
    tall = per * rows

    def step(t, _):
        qi = t // steps
        ci = t % steps

        @pl.when(qi == 0)
        def _():
            for b in range(per):
                i = ci * per + b
                pltpu.make_async_copy(kv_refs[0], kv_buf.at[pl.ds(i * rows, rows)], kv_sem.at[i]).wait()

        keys = pl.ds(pl.multiple_of(ci * tall, tall), tall)
        qa = q_buf[qi, :, 0 : 2 * wa]
        col = lax.broadcasted_iota(jnp.int32, qa.shape, 1)
        zero = jnp.zeros_like(qa)

        def score(j):
            if j < 2:
                q = jnp.where((col < wa) if j == 0 else (col >= wa), qa, zero)
                return dot(kv_buf[keys, 0 : 2 * wa], q, 1, 1)
            at = 2 * wa + (j - 2) * wb
            return dot(kv_buf[keys, at : at + wb], q_buf[qi, :, at : at + wb], 1, 1)

        s = score(0)
        for j in range(4):
            ahead = score(j + 1) if j < 3 else None
            c = consts[j // 2]
            old = ml_ref[qi, j : j + 1, :]
            top = jnp.maximum(old, jnp.max(s, axis=0, keepdims=True))
            w = jnp.exp2((s - top) * c)
            decay = jnp.exp2((old - top) * c)
            ml_ref[qi, j : j + 1, :] = top
            ml_ref[qi, j + 4 : j + 5, :] = ml_ref[qi, j + 4 : j + 5, :] * decay + jnp.sum(w, axis=0, keepdims=True)
            at = 2 * wa + 2 * wb + (j // 2) * vd
            more = dot(kv_buf[keys, at : at + vd], w.astype(bf16), 0, 0)
            part = slice(j * vd, (j + 1) * vd)
            acc_ref[qi, part, :] = acc_ref[qi, part, :] * decay + more
            s = ahead
        return 0

    lax.fori_loop(0, nq * steps, step, 0)
    if last:
        for j in range(4):
            part = slice(j * vd, (j + 1) * vd)
            inverse = 1.0 / ml_ref[0, j + 4 : j + 5, :]
            o_ref[part, :] = (acc_ref[0, part, :] * inverse).astype(bf16)


def attend(queries, blocks, state, last, consts, wa, wb, vd):
    nq, nk = len(queries), len(blocks)
    rows = queries[0].shape[0]
    wide = queries[0].shape[1]
    cols = blocks[0].shape[1]
    anywhere = pl.BlockSpec(memory_space=pl.ANY)
    vmem = pl.BlockSpec(memory_space=pltpu.VMEM)
    acc_shape = jax.ShapeDtypeStruct((nq, 4 * vd, rows), f32)
    ml_shape = jax.ShapeDtypeStruct((nq, 8, rows), f32)
    scratch = [
        pltpu.VMEM((nq, rows, wide), bf16),
        pltpu.VMEM((nk * rows, cols), bf16),
        pltpu.SemaphoreType.DMA((nq,)),
        pltpu.SemaphoreType.DMA((nk,)),
    ]
    if last:
        out_shape = (jax.ShapeDtypeStruct((4 * vd, rows), bf16), ml_shape)
        scratch.append(pltpu.VMEM((nq, 4 * vd, rows), f32))
    else:
        out_shape = (acc_shape, ml_shape)
    work = nq * nk * rows * rows
    return pl.pallas_call(
        functools.partial(attend_body, nq, nk, state is not None, last, consts, rows, wa, wb, vd),
        out_shape=out_shape,
        in_specs=[anywhere] * (nq + nk) + [vmem] * (0 if state is None else 2),
        out_specs=(vmem, vmem),
        scratch_shapes=scratch,
        compiler_params=pltpu.CompilerParams(vmem_limit_bytes=40 * 1024 * 1024),
        cost_estimate=pl.CostEstimate(flops=work * 4 * 4 * vd, transcendentals=4 * work, bytes_accessed=nk * rows * cols * 2),
        name="attend",
    )(*queries, *blocks, *(state or ()))


def merge_body(consts, vd, lam_ref, gain_ref, acc_ref, ml_ref, *refs):
    out_ref = refs[-1]
    others = [(refs[2 * i], refs[2 * i + 1]) for i in range((len(refs) - 1) // 2)]
    for g in range(2):
        ratio = []
        for j in (2 * g, 2 * g + 1):
            c = consts[g]
            part = slice(j * vd, (j + 1) * vd)
            tops = [ml_ref[0, j : j + 1, :]] + [m[0, j : j + 1, :] for _, m in others]
            sums = [ml_ref[0, j + 4 : j + 5, :]] + [m[0, j + 4 : j + 5, :] for _, m in others]
            top = functools.reduce(jnp.maximum, tops)
            decay = jnp.exp2((tops[0] - top) * c)
            numer = acc_ref[0, part, :] * decay
            denom = sums[0] * decay
            for (o, _), m, l in zip(others, tops[1:], sums[1:]):
                share = l * jnp.exp2((m - top) * c)
                denom = denom + share
                numer = numer + o[part, :].astype(f32) * share
            ratio.append(numer / denom)
        mixed = ratio[0] - lam_ref[g, 0] * ratio[1]
        inverse = lax.rsqrt(jnp.mean(mixed * mixed, axis=0, keepdims=True) + eps_norm)
        normed = mixed * inverse * gain_ref[:, g : g + 1] * head_scale
        out_ref[:, g * vd : (g + 1) * vd] = normed.T.astype(bf16)


def merge(state, others, lam, gain, consts, vd):
    rows = state[1].shape[-1]
    vmem = pl.BlockSpec(memory_space=pltpu.VMEM)
    smem = pl.BlockSpec(memory_space=pltpu.SMEM)
    flat = [a for pair in others for a in pair]
    return pl.pallas_call(
        functools.partial(merge_body, consts, vd),
        out_shape=jax.ShapeDtypeStruct((rows, 2 * vd), bf16),
        in_specs=[smem, vmem] + [vmem] * (2 + len(flat)),
        out_specs=vmem,
        compiler_params=pltpu.CompilerParams(vmem_limit_bytes=32 * 1024 * 1024),
        name="merge",
    )(lam, gain.T, *state, *flat)


def project_body(n, share, *refs):
    at_ref, heads, outs = refs[0], refs[1 : 1 + n], refs[1 + n : 1 + 2 * n]
    residual_ref, gain_ref, normed_ref, cols_ref, summed_ref = refs[1 + 2 * n :]
    total = residual_ref[...].astype(f32)
    for h, o in zip(heads, outs):
        total = total + dot(h[...], o[...], 1, 0)
    summed_ref[...] = total
    inverse = lax.rsqrt(jnp.mean(total * total, axis=-1, keepdims=True) + eps_norm)
    normed_ref[...] = (summed_ref[...] * inverse * gain_ref[...]).astype(bf16)
    cols_ref[...] = summed_ref[:, pl.ds(pl.multiple_of(at_ref[0] * share, share), share)]


def project(at, heads, outs, residual, gain, share):
    n = len(heads)
    rows, wide = residual.shape
    vmem = pl.BlockSpec(memory_space=pltpu.VMEM)
    smem = pl.BlockSpec(memory_space=pltpu.SMEM)
    return pl.pallas_call(
        functools.partial(project_body, n, share),
        out_shape=(jax.ShapeDtypeStruct((rows, wide), bf16), jax.ShapeDtypeStruct((rows, share), f32)),
        in_specs=[smem] + [vmem] * (2 * n + 2),
        out_specs=(vmem, vmem),
        scratch_shapes=[pltpu.VMEM((rows, wide), f32)],
        compiler_params=pltpu.CompilerParams(vmem_limit_bytes=40 * 1024 * 1024),
        cost_estimate=pl.CostEstimate(flops=2 * rows * wide * n * heads[0].shape[1], transcendentals=0, bytes_accessed=8 * 1024 * 1024),
        name="project",
    )(at, *heads, *outs, residual, gain)


def ffn_body(n, at_ref, x_ref, w_ref, *refs):
    outs, gate_ref, hidden_ref = refs[:n], refs[n], refs[n + 1]
    which = pl.program_id(0)
    spread, _, deep, units = w_ref.shape

    @pl.when(which == 0)
    def _():
        gate_ref[...] = dot(x_ref[...], w_ref[...].reshape(spread * deep, units), 1, 0)

    @pl.when(which == 1)
    def _():
        up = dot(x_ref[...], w_ref[...].reshape(spread * deep, units), 1, 0)
        gate = gate_ref[...]
        hidden_ref[...] = (gate / (1.0 + jnp.exp(-gate)) * up).astype(bf16)

    @pl.when(which == 2)
    def _():
        part = spread // n
        for k in range(n):
            j = (at_ref[0] + k) % n
            w = w_ref[pl.ds(j * part, part), 0].reshape(part * deep, units)
            outs[k][...] = dot(hidden_ref[...], w, 1, 1).astype(bf16)


def ffn(at, x, w, n):
    rows, wide = x.shape
    spread, three, deep, units = w.shape
    share = wide // n
    smem = pl.BlockSpec(memory_space=pltpu.SMEM)
    out = pl.BlockSpec((rows, share), lambda p: (0, 0))
    return pl.pallas_call(
        functools.partial(ffn_body, n),
        grid=(three,),
        out_shape=(jax.ShapeDtypeStruct((rows, share), bf16),) * n,
        in_specs=[
            smem,
            pl.BlockSpec((rows, wide), lambda p: (0, 0)),
            pl.BlockSpec((spread, 1, deep, units), lambda p: (0, p, 0, 0)),
        ],
        out_specs=(out,) * n,
        scratch_shapes=[pltpu.VMEM((rows, units), f32), pltpu.VMEM((rows, units), bf16)],
        compiler_params=pltpu.CompilerParams(vmem_limit_bytes=50 * 1024 * 1024, dimension_semantics=("arbitrary",)),
        cost_estimate=pl.CostEstimate(flops=6 * rows * wide * units, transcendentals=rows * units, bytes_accessed=w.size * 2),
        name="ffn",
    )(at, x, w)


def local(
    residual,
    queries_a,
    keys_a,
    values_a,
    queries_b,
    keys_b,
    values_b,
    mix_lambda,
    head_gain,
    out_a,
    out_b,
    norm_gain,
    w_gate,
    w_up,
    w_down,
):
    wa = queries_a.shape[1] // 2
    wb = queries_b.shape[1] // 2
    vd = values_a.shape[1]
    consts = (wa**-0.5 * log2e, wb**-0.5 * log2e)
    n = lax.axis_size("tp")
    share = residual.shape[1] // n
    at = lax.axis_index("tp").astype(jnp.int32)[None]

    kv = jnp.concatenate([keys_a, keys_b, values_a, values_b], axis=1)
    q = jnp.concatenate([queries_a, queries_b], axis=1)
    queries = [q] + [along_y(q, k) for k in range(1, 4)]
    near = [kv] + [along_z(kv, k) for k in range(1, 4)]
    far = [other_core(b) for b in near]
    oo = jnp.concatenate([out_a, out_b], axis=0)
    outs = [oo] + [along_x(oo, k) for k in range(1, 4)]
    weights = lax.all_gather(jnp.stack([w_gate, w_up, w_down.T]), "sp", axis=0)

    go = functools.partial(attend, consts=consts, wa=wa, wb=wb, vd=vd)
    here = [near[0], far[0]]
    away = [b for k in (1, 3, 2) for b in (near[k], far[k])]
    own = go(queries[:1], here, None, False)
    rest = go(queries[1:], here, None, False)
    back = {}
    for k in (2, 1, 3):
        part = tuple(a[k - 1 : k] for a in rest)
        o, ml = go(queries[k : k + 1], away, part, True)
        back[k] = (along_y(o, -k), along_y(ml, -k))
    own = go(queries[:1], away, own, False)
    heads = merge(own, [back[k] for k in (1, 3, 2)], mix_lambda, head_gain, consts, vd)

    everyone = [heads] + [along_x(heads, k) for k in range(1, 4)]
    normed, cols = project(at, everyone, outs, residual, norm_gain[None], share)
    pieces = ffn(at, normed, weights, n)
    arrived = [along_x(pieces[k], k) for k in range(1, n)]
    channel = pieces[0].astype(f32)
    for a in arrived:
        channel = channel + a.astype(f32)
    return (cols + 0.5 * channel).astype(bf16)


def solution(mesh):
    in_specs = (
        P("sp", None),
        P("sp", "tp"),
        P("sp", "tp"),
        P("sp", "tp"),
        P("sp", "tp"),
        P("sp", "tp"),
        P("sp", "tp"),
        P(None, "tp"),
        P(),
        P("tp", None),
        P("tp", None),
        P(),
        P("sp", "tp"),
        P("sp", "tp"),
        P("tp", "sp"),
    )
    out_specs = P("sp", "tp")
    return jax.shard_map(local, mesh=mesh, in_specs=in_specs, out_specs=out_specs, check_vma=False)
```

```python
import math
import functools
import jax
import jax.numpy as jnp
from jax import lax
from jax.experimental import pallas as pl
from jax.experimental.pallas import tpu as pltpu
from jax.sharding import PartitionSpec as P

eps_norm = 1e-06
head_scale = 0.8
log2e = math.log2(math.e)
f32 = jnp.float32
bf16 = jnp.bfloat16

SP = [(z, y, c) for z in range(4) for y in range(4) for c in range(2)]


def place(z, y, c):
    return (z % 4) * 8 + (y % 4) * 2 + c % 2


def along_y(x, k):
    return lax.ppermute(x, "sp", [(place(z, y, c), place(z, y + k, c)) for z, y, c in SP])


def along_z(x, k):
    return lax.ppermute(x, "sp", [(place(z, y, c), place(z + k, y, c)) for z, y, c in SP])


def other_core(x):
    return lax.ppermute(x, "sp", [(place(z, y, c), place(z, y, c + 1)) for z, y, c in SP])


def along_x(x, k):
    return lax.ppermute(x, "tp", [(i, (i + k) % 4) for i in range(4)])


def dot(a, b, ca, cb):
    return lax.dot_general(a, b, (((ca,), (cb,)), ((), ())), preferred_element_type=f32)


PER = 2
MIB = 1024 * 1024


def attend_body(groups, m, nk, carry, pick, consts, rows, wa, wb, vd, *refs):
    nq = groups * m
    q_refs, refs = refs[:nq], refs[nq:]
    kv_refs, refs = refs[:nk], refs[nk:]
    if carry:
        acc_in, ml_in, refs = refs[0], refs[1], refs[2:]
    send = pick is not None and pick[2]
    if send:
        o_ref, q_buf, kv_buf, q_sem, kv_sem, acc_sem, acc_ref, ml_ref = refs
    else:
        acc_ref, ml_ref, q_buf, kv_buf, q_sem, kv_sem, acc_sem = refs
    q_copies = [
        pltpu.make_async_copy(q_refs[i], q_buf.at[i // m, pl.ds((i % m) * rows, rows)], q_sem.at[i]) for i in range(nq)
    ]
    kv_copies = [
        pltpu.make_async_copy(kv_refs[i], kv_buf.at[pl.ds(i * rows, rows)], kv_sem.at[i]) for i in range(nk)
    ]
    if carry:
        if pick is not None:
            lanes = pl.ds(pick[1] * rows, rows)
            acc_in = acc_in.at[pl.ds(pick[0], 1), :, lanes]
            ml_in = ml_in.at[pl.ds(pick[0], 1), :, lanes]
        acc_copies = [
            pltpu.make_async_copy(acc_in, acc_ref, acc_sem.at[0]),
            pltpu.make_async_copy(ml_in, ml_ref, acc_sem.at[1]),
        ]
    else:
        acc_copies = []
    per = min(PER, nk) if m == 1 else 1
    for c in q_copies + kv_copies[:per] + acc_copies + kv_copies[per:]:
        c.start()
    if not carry:
        acc_ref[...] = jnp.zeros_like(acc_ref)
        ml_ref[:, 0:8, :] = jnp.full((groups, 8, m * rows), -jnp.inf, f32)
        ml_ref[:, 8:16, :] = jnp.zeros((groups, 8, m * rows), f32)
    for c in q_copies + acc_copies:
        c.wait()
    steps = nk // per
    tall = per * rows

    def step(t, _):
        qi = t // steps
        ci = t % steps

        @pl.when(qi == 0)
        def _():
            for b in range(per):
                i = ci * per + b
                pltpu.make_async_copy(kv_refs[0], kv_buf.at[pl.ds(i * rows, rows)], kv_sem.at[i]).wait()

        keys = pl.ds(pl.multiple_of(ci * tall, tall), tall)
        qa = q_buf[qi, :, 0 : 2 * wa]
        col = lax.broadcasted_iota(jnp.int32, qa.shape, 1)
        zero = jnp.zeros_like(qa)

        def score(j):
            if j < 2:
                q = jnp.where((col < wa) if j == 0 else (col >= wa), qa, zero)
                return dot(kv_buf[keys, 0 : 2 * wa], q, 1, 1)
            at = 2 * wa + (j - 2) * wb
            return dot(kv_buf[keys, at : at + wb], q_buf[qi, :, at : at + wb], 1, 1)

        s = score(0)
        for j in range(4):
            ahead = score(j + 1) if j < 3 else None
            c = consts[j // 2]
            old = ml_ref[qi, j : j + 1, :]
            top = jnp.maximum(old, jnp.max(s, axis=0, keepdims=True))
            w = jnp.exp2((s - top) * c)
            decay = jnp.exp2((old - top) * c)
            ml_ref[qi, j : j + 1, :] = top
            ml_ref[qi, j + 8 : j + 9, :] = ml_ref[qi, j + 8 : j + 9, :] * decay + jnp.sum(w, axis=0, keepdims=True)
            at = 2 * wa + 2 * wb + (j // 2) * vd
            more = dot(kv_buf[keys, at : at + vd], w.astype(bf16), 0, 0)
            part = slice(j * vd, (j + 1) * vd)
            acc_ref[qi, part, :] = acc_ref[qi, part, :] * decay + more
            s = ahead
        return 0

    lax.fori_loop(0, groups * steps, step, 0)
    if send:
        for j in range(4):
            part = slice(j * vd, (j + 1) * vd)
            inverse = 1.0 / ml_ref[0, j + 8 : j + 9, :]
            o_ref[part, :] = (acc_ref[0, part, :] * inverse).astype(bf16)
        level = level_of(ml_ref, consts)
        high = level.astype(bf16).astype(f32)
        mid = (level - high).astype(bf16).astype(f32)
        low = level - high - mid
        o_ref[4 * vd :, :] = jnp.concatenate([high, mid, low, jnp.zeros_like(low)], axis=0).astype(bf16)


def level_of(ml_ref, consts):
    row = lax.broadcasted_iota(jnp.int32, (8, ml_ref.shape[2]), 0)
    used = row < 4
    top = jnp.where(used, ml_ref[0, 0:8, :], 0.0)
    total = jnp.where(used, ml_ref[0, 8:16, :], 1.0)
    return top * jnp.where(row < 2, consts[0], consts[1]) + jnp.log2(total)


def attend(queries, blocks, state, pick, consts, wa, wb, vd):
    groups, m = len(queries), len(queries[0])
    flat = [q for g in queries for q in g]
    nq, nk = len(flat), len(blocks)
    rows = flat[0].shape[0]
    wide = flat[0].shape[1]
    cols = blocks[0].shape[1]
    anywhere = pl.BlockSpec(memory_space=pl.ANY)
    vmem = pl.BlockSpec(memory_space=pltpu.VMEM)
    acc_shape = (groups, 4 * vd, m * rows)
    ml_shape = (groups, 16, m * rows)
    scratch = [
        pltpu.VMEM((groups, m * rows, wide), bf16),
        pltpu.VMEM((nk * rows, cols), bf16),
        pltpu.SemaphoreType.DMA((nq,)),
        pltpu.SemaphoreType.DMA((nk,)),
        pltpu.SemaphoreType.DMA((2,)),
    ]
    if pick is not None and pick[2]:
        out_shape = jax.ShapeDtypeStruct((4 * vd + 32, rows), bf16)
        out_specs = vmem
        scratch += [pltpu.VMEM(acc_shape, f32), pltpu.VMEM(ml_shape, f32)]
    else:
        out_shape = (jax.ShapeDtypeStruct(acc_shape, f32), jax.ShapeDtypeStruct(ml_shape, f32))
        out_specs = (vmem, vmem)
    work = nq * nk * rows * rows
    return pl.pallas_call(
        functools.partial(attend_body, groups, m, nk, state is not None, pick, consts, rows, wa, wb, vd),
        out_shape=out_shape,
        in_specs=[anywhere] * (nq + nk + (0 if state is None else 2)),
        out_specs=out_specs,
        scratch_shapes=scratch,
        compiler_params=pltpu.CompilerParams(vmem_limit_bytes=(14 if m > 1 else 10) * MIB),
        cost_estimate=pl.CostEstimate(flops=work * 4 * 4 * vd, transcendentals=4 * work, bytes_accessed=nk * rows * cols * 2),
        name="attend",
    )(*flat, *blocks, *(state or ()))


def merge_body(consts, vd, lam_ref, gain_ref, acc_ref, ml_ref, *refs):
    others, out_ref = refs[:-1], refs[-1]
    levels = [level_of(ml_ref, consts)]
    for o in others:
        stats = o[4 * vd :, :].astype(f32)
        levels.append(stats[0:8] + stats[8:16] + stats[16:24])
    top = functools.reduce(jnp.maximum, levels)
    shares = [jnp.exp2(v - top) for v in levels]
    inverse = 1.0 / functools.reduce(jnp.add, shares)
    shares = [v * inverse for v in shares]
    for g in range(2):
        ratio = []
        for j in (2 * g, 2 * g + 1):
            part = slice(j * vd, (j + 1) * vd)
            value = acc_ref[0, part, :] * (shares[0][j : j + 1] / ml_ref[0, j + 8 : j + 9, :])
            for o, share in zip(others, shares[1:]):
                value = value + o[part, :].astype(f32) * share[j : j + 1]
            ratio.append(value)
        mixed = ratio[0] - lam_ref[g, 0] * ratio[1]
        scale = lax.rsqrt(jnp.mean(mixed * mixed, axis=0, keepdims=True) + eps_norm)
        normed = mixed * scale * gain_ref[:, g : g + 1] * head_scale
        out_ref[:, g * vd : (g + 1) * vd] = normed.T.astype(bf16)


def merge(state, others, lam, gain, consts, vd):
    rows = state[1].shape[-1]
    vmem = pl.BlockSpec(memory_space=pltpu.VMEM)
    smem = pl.BlockSpec(memory_space=pltpu.SMEM)
    return pl.pallas_call(
        functools.partial(merge_body, consts, vd),
        out_shape=jax.ShapeDtypeStruct((rows, 2 * vd), bf16),
        in_specs=[smem, vmem] + [vmem] * (2 + len(others)),
        out_specs=vmem,
        compiler_params=pltpu.CompilerParams(vmem_limit_bytes=12 * MIB),
        name="merge",
    )(lam, gain.T, *state, *others)


def project_body(n, share, *refs):
    at_ref, heads, outs = refs[0], refs[1 : 1 + n], refs[1 + n : 1 + 2 * n]
    residual_ref, gain_ref, normed_ref, cols_ref, summed_ref = refs[1 + 2 * n :]
    total = residual_ref[...].astype(f32)
    for h, o in zip(heads, outs):
        total = total + dot(h[...], o[...], 1, 0)
    summed_ref[...] = total
    inverse = lax.rsqrt(jnp.mean(total * total, axis=-1, keepdims=True) + eps_norm)
    normed_ref[...] = (summed_ref[...] * inverse * gain_ref[...]).astype(bf16)
    cols_ref[...] = summed_ref[:, pl.ds(pl.multiple_of(at_ref[0] * share, share), share)]


def project(at, heads, outs, residual, gain, share):
    n = len(heads)
    rows, wide = residual.shape
    vmem = pl.BlockSpec(memory_space=pltpu.VMEM)
    smem = pl.BlockSpec(memory_space=pltpu.SMEM)
    return pl.pallas_call(
        functools.partial(project_body, n, share),
        out_shape=(jax.ShapeDtypeStruct((rows, wide), bf16), jax.ShapeDtypeStruct((rows, share), f32)),
        in_specs=[smem] + [vmem] * (2 * n + 2),
        out_specs=(vmem, vmem),
        scratch_shapes=[pltpu.VMEM((rows, wide), f32)],
        compiler_params=pltpu.CompilerParams(vmem_limit_bytes=20 * MIB),
        cost_estimate=pl.CostEstimate(flops=2 * rows * wide * n * heads[0].shape[1], transcendentals=0, bytes_accessed=8 * MIB),
        name="project",
    )(at, *heads, *outs, residual, gain)


def ffn_body(n, x_ref, w_ref, out_ref, gate_ref, hidden_ref):
    which = pl.program_id(0)
    spread, _, deep, units = w_ref.shape

    @pl.when(which == 0)
    def _():
        gate_ref[...] = dot(x_ref[...], w_ref[...].reshape(spread * deep, units), 1, 0)

    @pl.when(which == 1)
    def _():
        up = dot(x_ref[...], w_ref[...].reshape(spread * deep, units), 1, 0)
        gate = gate_ref[...]
        hidden_ref[...] = (gate / (1.0 + jnp.exp(-gate)) * up).astype(bf16)

    @pl.when(which == 2)
    def _():
        part = spread // n
        for k in range(n):
            w = w_ref[k * part : (k + 1) * part, 0].reshape(part * deep, units)
            out_ref[k] = dot(hidden_ref[...], w, 1, 1).astype(bf16)


def ffn(x, w, n):
    rows, wide = x.shape
    spread, three, deep, units = w.shape
    share = wide // n
    return pl.pallas_call(
        functools.partial(ffn_body, n),
        grid=(three,),
        out_shape=jax.ShapeDtypeStruct((n, rows, share), bf16),
        in_specs=[
            pl.BlockSpec((rows, wide), lambda p: (0, 0)),
            pl.BlockSpec((spread, 1, deep, units), lambda p: (0, p, 0, 0)),
        ],
        out_specs=pl.BlockSpec((n, rows, share), lambda p: (0, 0, 0)),
        scratch_shapes=[pltpu.VMEM((rows, units), f32), pltpu.VMEM((rows, units), bf16)],
        compiler_params=pltpu.CompilerParams(vmem_limit_bytes=36 * MIB, dimension_semantics=("arbitrary",)),
        cost_estimate=pl.CostEstimate(flops=6 * rows * wide * units, transcendentals=rows * units, bytes_accessed=w.size * 2),
        name="ffn",
    )(x, w)


def local(
    residual,
    queries_a,
    keys_a,
    values_a,
    queries_b,
    keys_b,
    values_b,
    mix_lambda,
    head_gain,
    out_a,
    out_b,
    norm_gain,
    w_gate,
    w_up,
    w_down,
):
    wa = queries_a.shape[1] // 2
    wb = queries_b.shape[1] // 2
    vd = values_a.shape[1]
    consts = (wa**-0.5 * log2e, wb**-0.5 * log2e)
    n = lax.axis_size("tp")
    share = residual.shape[1] // n
    at = lax.axis_index("tp").astype(jnp.int32)[None]

    kv = jnp.concatenate([keys_a, keys_b, values_a, values_b], axis=1)
    q = jnp.concatenate([queries_a, queries_b], axis=1)
    near = [kv] + [along_z(kv, k) for k in range(1, 4)]
    queries = [q] + [along_y(q, k) for k in range(1, 4)]
    kv_far = other_core(kv)
    oo = jnp.concatenate([out_a, out_b], axis=0)
    outs = [oo] + [along_x(oo, k) for k in range(1, 4)]
    weights = lax.all_gather(jnp.stack([w_gate, w_up, w_down.T]), "sp", axis=0)

    go = functools.partial(attend, consts=consts, wa=wa, wb=wb, vd=vd)
    order = ((2, 1), (3, 0))
    pairs = [[queries[k] for k in g] for g in order]
    state = go(pairs, [kv, kv_far], None, None)
    one, three, *state = lax.optimization_barrier((near[1], near[3], *state))
    far = {1: other_core(one), 3: other_core(three)}
    state = go(pairs, [one, three], state, None)
    two, one, three, *state = lax.optimization_barrier((near[2], far[1], far[3], *state))
    last = [two, other_core(two)]
    state = go(pairs, [one, three], state, None)
    back = {}
    for g, group in enumerate(order):
        for i, k in enumerate(group):
            done = go([[queries[k]]], last, state, (g, i, k != 0))
            if k:
                back[k] = along_y(done, -k)
            else:
                own = done
    heads = merge(own, [back[k] for k in (1, 3, 2)], mix_lambda, head_gain, consts, vd)

    everyone = [heads] + [along_x(heads, k) for k in range(1, 4)]
    normed, cols = project(at, everyone, outs, residual, norm_gain[None], share)
    pieces = lax.all_to_all(ffn(normed, weights, n), "tp", 0, 0, tiled=True)
    return (cols + 0.5 * pieces.astype(f32).sum(axis=0)).astype(bf16)


def solution(mesh):
    in_specs = (
        P("sp", None),
        P("sp", "tp"),
        P("sp", "tp"),
        P("sp", "tp"),
        P("sp", "tp"),
        P("sp", "tp"),
        P("sp", "tp"),
        P(None, "tp"),
        P(),
        P("tp", None),
        P("tp", None),
        P(),
        P("sp", "tp"),
        P("sp", "tp"),
        P("tp", "sp"),
    )
    out_specs = P("sp", "tp")
    return jax.shard_map(local, mesh=mesh, in_specs=in_specs, out_specs=out_specs, check_vma=False)
```

```python
import math
import functools
import jax
import jax.numpy as jnp
from jax import lax
from jax.experimental import pallas as pl
from jax.experimental.pallas import tpu as pltpu
from jax.sharding import PartitionSpec as P

eps_norm = 1e-06
head_scale = 0.8
log2e = math.log2(math.e)
f32 = jnp.float32
bf16 = jnp.bfloat16

SP = [(z, y, c) for z in range(4) for y in range(4) for c in range(2)]


def place(z, y, c):
    return (z % 4) * 8 + (y % 4) * 2 + c % 2


def along_y(x, k):
    return lax.ppermute(x, "sp", [(place(z, y, c), place(z, y + k, c)) for z, y, c in SP])


def along_z(x, k):
    return lax.ppermute(x, "sp", [(place(z, y, c), place(z + k, y, c)) for z, y, c in SP])


def other_core(x):
    return lax.ppermute(x, "sp", [(place(z, y, c), place(z, y, c + 1)) for z, y, c in SP])


def along_x(x, k):
    return lax.ppermute(x, "tp", [(i, (i + k) % 4) for i in range(4)])


def dot(a, b, ca, cb):
    return lax.dot_general(a, b, (((ca,), (cb,)), ((), ())), preferred_element_type=f32)


def pack_body(layout, *refs):
    n = sum(len(parts) for parts in layout)
    ins, outs, sem = refs[:n], refs[n:-1], refs[-1]
    copies, i = [], 0
    for out, parts in zip(outs, layout):
        for corner in parts:
            part = tuple(pl.ds(c, d) for c, d in zip(corner, ins[i].shape))
            copies.append(pltpu.make_async_copy(ins[i], out.at[part], sem.at[i]))
            i += 1
    for c in copies:
        c.start()
    for c in copies:
        c.wait()


def in_hbm(x):
    return pltpu.with_memory_space_constraint(x, pltpu.HBM)


def pack(*sides):
    layout, shapes = [], []
    for arrays, axis in sides:
        at, corners = 0, []
        for a in arrays:
            corners.append((at, 0) if axis == 0 else (0, at))
            at += a.shape[axis]
        other = arrays[0].shape[1 - axis]
        layout.append(corners)
        shapes.append(jax.ShapeDtypeStruct((at, other) if axis == 0 else (other, at), arrays[0].dtype))
    flat = [in_hbm(a) for arrays, _ in sides for a in arrays]
    return pl.pallas_call(
        functools.partial(pack_body, layout),
        out_shape=tuple(shapes),
        in_specs=[pl.BlockSpec(memory_space=pltpu.HBM)] * len(flat),
        out_specs=tuple(pl.BlockSpec(memory_space=pltpu.VMEM) for _ in shapes),
        scratch_shapes=[pltpu.SemaphoreType.DMA((len(flat),))],
        compiler_params=pltpu.CompilerParams(vmem_limit_bytes=8 * MIB),
        name="pack",
    )(*flat)


PER = 2
AHEAD = 3
MIB = 1024 * 1024


def attend_body(groups, m, nk, carry, pick, consts, rows, wa, wb, vd, *refs):
    nq = groups * m
    q_refs, refs = refs[:nq], refs[nq:]
    kv_refs, refs = refs[:nk], refs[nk:]
    if carry:
        acc_in, ml_in, refs = refs[0], refs[1], refs[2:]
    send = pick is not None and pick[2]
    outs = 1 if send else 2
    q_buf, kv_buf, pad_buf, q_sem, kv_sem, acc_sem = refs[outs : outs + 6]
    turned = None
    rest = refs[outs + 6 :]
    if groups > 1:
        turned, rest = rest[0], rest[1:]
    if send:
        o_ref = refs[0]
        acc_ref, ml_ref = rest
    else:
        acc_ref, ml_ref = refs[:2]
    q_copies = [
        pltpu.make_async_copy(q_refs[i], q_buf.at[i // m, pl.ds((i % m) * rows, rows)], q_sem.at[i]) for i in range(nq)
    ]
    kv_copies = [
        pltpu.make_async_copy(kv_refs[i], kv_buf.at[pl.ds(i * rows, rows)], kv_sem.at[i]) for i in range(nk)
    ]
    if carry:
        if pick is not None:
            lanes = pl.ds(pick[1] * rows, rows)
            acc_in = acc_in.at[pl.ds(pick[0], 1), :, lanes]
            ml_in = ml_in.at[pl.ds(pick[0], 1), :, lanes]
        acc_copies = [
            pltpu.make_async_copy(acc_in, acc_ref, acc_sem.at[0]),
            pltpu.make_async_copy(ml_in, ml_ref, acc_sem.at[1]),
        ]
    else:
        acc_copies = []
    per = min(PER, nk)
    for c in q_copies + kv_copies[:per] + acc_copies + kv_copies[per:]:
        c.start()
    if not carry:
        acc_ref[...] = jnp.zeros_like(acc_ref)
        ml_ref[:, 0:8, :] = jnp.full((groups, 8, m * rows), -jnp.inf, f32)
        ml_ref[:, 8:16, :] = jnp.zeros((groups, 8, m * rows), f32)
    for c in q_copies:
        c.wait()
    for g in range(groups):
        qa = q_buf[g, :, 0 : 2 * wa]
        col = lax.broadcasted_iota(jnp.int32, qa.shape, 1)
        zero = jnp.zeros_like(qa)
        pad_buf[g, :, 0 : 2 * wa] = jnp.where(col < wa, qa, zero)
        pad_buf[g, :, 2 * wa :] = jnp.where(col >= wa, qa, zero)
    for c in acc_copies:
        c.wait()
    steps = nk // per
    tall = per * rows
    wide = m * rows
    lane = 256 if wide % 256 == 0 else wide
    items = [(h, j) for h in range(wide // lane) for j in range(4)]

    def step(t, _):
        qi = t // steps
        ci = t % steps
        keys = pl.ds(pl.multiple_of(ci * tall, tall), tall)

        @pl.when(qi == 0)
        def _():
            for b in range(per):
                i = ci * per + b
                pltpu.make_async_copy(kv_refs[0], kv_buf.at[pl.ds(i * rows, rows)], kv_sem.at[i]).wait()
            if turned is not None:
                first = lax.broadcasted_iota(jnp.int32, (16, tall), 0) == 0
                for g in range(2):
                    at = 2 * wa + 2 * wb + g * vd
                    turned[ci, g, 0:vd, :] = kv_buf[keys, at : at + vd].T
                    turned[ci, g, vd : vd + 16, :] = jnp.where(first, 1.0, 0.0).astype(bf16)

        def score(h, j):
            lanes = slice(h * lane, (h + 1) * lane)
            if j < 2:
                return dot(kv_buf[keys, 0 : 2 * wa], pad_buf[qi, lanes, j * 2 * wa : (j + 1) * 2 * wa], 1, 1)
            at = 2 * wa + (j - 2) * wb
            return dot(kv_buf[keys, at : at + wb], q_buf[qi, lanes, at : at + wb], 1, 1)

        ready = [score(*item) for item in items[:AHEAD]]
        for n, (h, j) in enumerate(items):
            if n + AHEAD < len(items):
                ready.append(score(*items[n + AHEAD]))
            s = ready.pop(0)
            lanes = slice(h * lane, (h + 1) * lane)
            c = consts[j // 2]
            old = ml_ref[qi, j : j + 1, lanes]
            top = jnp.maximum(old, jnp.max(s, axis=0, keepdims=True))
            w = jnp.exp2((s - top) * c)
            decay = jnp.exp2((old - top) * c)
            ml_ref[qi, j : j + 1, lanes] = top
            if turned is not None:
                more = dot(turned[ci, j // 2], w.astype(bf16), 1, 0)
                total = more[vd : vd + 1]
                more = more[0:vd]
            else:
                total = jnp.sum(w, axis=0, keepdims=True)
                at = 2 * wa + 2 * wb + (j // 2) * vd
                more = dot(kv_buf[keys, at : at + vd], w.astype(bf16), 0, 0)
            ml_ref[qi, j + 8 : j + 9, lanes] = ml_ref[qi, j + 8 : j + 9, lanes] * decay + total
            part = slice(j * vd, (j + 1) * vd)
            acc_ref[qi, part, lanes] = acc_ref[qi, part, lanes] * decay + more
        return 0

    lax.fori_loop(0, groups * steps, step, 0)
    if send:
        for j in range(4):
            part = slice(j * vd, (j + 1) * vd)
            inverse = 1.0 / ml_ref[0, j + 8 : j + 9, :]
            o_ref[part, :] = (acc_ref[0, part, :] * inverse).astype(bf16)
        level = level_of(ml_ref, consts)
        high = level.astype(bf16).astype(f32)
        mid = (level - high).astype(bf16).astype(f32)
        low = level - high - mid
        o_ref[4 * vd :, :] = jnp.concatenate([high, mid, low, jnp.zeros_like(low)], axis=0).astype(bf16)


def level_of(ml_ref, consts):
    row = lax.broadcasted_iota(jnp.int32, (8, ml_ref.shape[2]), 0)
    used = row < 4
    top = jnp.where(used, ml_ref[0, 0:8, :], 0.0)
    total = jnp.where(used, ml_ref[0, 8:16, :], 1.0)
    return top * jnp.where(row < 2, consts[0], consts[1]) + jnp.log2(total)


def attend(queries, blocks, state, pick, consts, wa, wb, vd):
    groups, m = len(queries), len(queries[0])
    flat = [q for g in queries for q in g]
    nq, nk = len(flat), len(blocks)
    rows = flat[0].shape[0]
    wide = flat[0].shape[1]
    cols = blocks[0].shape[1]
    anywhere = pl.BlockSpec(memory_space=pl.ANY)
    vmem = pl.BlockSpec(memory_space=pltpu.VMEM)
    acc_shape = (groups, 4 * vd, m * rows)
    ml_shape = (groups, 16, m * rows)
    scratch = [
        pltpu.VMEM((groups, m * rows, wide), bf16),
        pltpu.VMEM((nk * rows, cols), bf16),
        pltpu.VMEM((groups, m * rows, 4 * wa), bf16),
        pltpu.SemaphoreType.DMA((nq,)),
        pltpu.SemaphoreType.DMA((nk,)),
        pltpu.SemaphoreType.DMA((2,)),
    ]
    if groups > 1:
        per = min(PER, nk)
        scratch.append(pltpu.VMEM((nk // per, 2, vd + 16, per * rows), bf16))
    if pick is not None and pick[2]:
        out_shape = jax.ShapeDtypeStruct((4 * vd + 32, rows), bf16)
        out_specs = vmem
        scratch += [pltpu.VMEM(acc_shape, f32), pltpu.VMEM(ml_shape, f32)]
    else:
        out_shape = (jax.ShapeDtypeStruct(acc_shape, f32), jax.ShapeDtypeStruct(ml_shape, f32))
        out_specs = (vmem, vmem)
    work = nq * nk * rows * rows
    return pl.pallas_call(
        functools.partial(attend_body, groups, m, nk, state is not None, pick, consts, rows, wa, wb, vd),
        out_shape=out_shape,
        in_specs=[anywhere] * (nq + nk + (0 if state is None else 2)),
        out_specs=out_specs,
        scratch_shapes=scratch,
        compiler_params=pltpu.CompilerParams(vmem_limit_bytes=16 * MIB),
        cost_estimate=pl.CostEstimate(flops=work * 4 * 4 * vd, transcendentals=4 * work, bytes_accessed=nk * rows * cols * 2),
        name="attend",
    )(*flat, *blocks, *(state or ()))


def merge_body(consts, vd, lam_ref, gain_ref, acc_ref, ml_ref, *refs):
    others, out_ref = refs[:-1], refs[-1]
    levels = [level_of(ml_ref, consts)]
    for o in others:
        stats = o[4 * vd :, :].astype(f32)
        levels.append(stats[0:8] + stats[8:16] + stats[16:24])
    top = functools.reduce(jnp.maximum, levels)
    shares = [jnp.exp2(v - top) for v in levels]
    inverse = 1.0 / functools.reduce(jnp.add, shares)
    shares = [v * inverse for v in shares]
    for g in range(2):
        ratio = []
        for j in (2 * g, 2 * g + 1):
            part = slice(j * vd, (j + 1) * vd)
            value = acc_ref[0, part, :] * (shares[0][j : j + 1] / ml_ref[0, j + 8 : j + 9, :])
            for o, share in zip(others, shares[1:]):
                value = value + o[part, :].astype(f32) * share[j : j + 1]
            ratio.append(value)
        mixed = ratio[0] - lam_ref[0:1, g : g + 1] * ratio[1]
        scale = lax.rsqrt(jnp.mean(mixed * mixed, axis=0, keepdims=True) + eps_norm)
        normed = (mixed * scale).T * gain_ref[g : g + 1, :] * head_scale
        out_ref[:, g * vd : (g + 1) * vd] = normed.astype(bf16)


def merge(state, others, lam, gain, consts, vd):
    rows = state[1].shape[-1]
    vmem = pl.BlockSpec(memory_space=pltpu.VMEM)
    return pl.pallas_call(
        functools.partial(merge_body, consts, vd),
        out_shape=jax.ShapeDtypeStruct((rows, 2 * vd), bf16),
        in_specs=[vmem] * (4 + len(others)),
        out_specs=vmem,
        compiler_params=pltpu.CompilerParams(vmem_limit_bytes=12 * MIB),
        name="merge",
    )(lam.T, gain, *state, *others)


def project_body(n, share, *refs):
    at_ref, heads, outs = refs[0], refs[1 : 1 + n], refs[1 + n : 1 + 2 * n]
    residual_ref, gain_ref, normed_ref, cols_ref, summed_ref = refs[1 + 2 * n :]
    total = residual_ref[...].astype(f32)
    for h, o in zip(heads, outs):
        total = total + dot(h[...], o[...], 1, 0)
    summed_ref[...] = total
    inverse = lax.rsqrt(jnp.mean(total * total, axis=-1, keepdims=True) + eps_norm)
    normed_ref[...] = (summed_ref[...] * inverse * gain_ref[...]).astype(bf16)
    cols_ref[...] = summed_ref[:, pl.ds(pl.multiple_of(at_ref[0] * share, share), share)]


def project(at, heads, outs, residual, gain, share):
    n = len(heads)
    rows, wide = residual.shape
    vmem = pl.BlockSpec(memory_space=pltpu.VMEM)
    smem = pl.BlockSpec(memory_space=pltpu.SMEM)
    return pl.pallas_call(
        functools.partial(project_body, n, share),
        out_shape=(jax.ShapeDtypeStruct((rows, wide), bf16), jax.ShapeDtypeStruct((rows, share), f32)),
        in_specs=[smem] + [vmem] * (2 * n + 2),
        out_specs=(vmem, vmem),
        scratch_shapes=[pltpu.VMEM((rows, wide), f32)],
        compiler_params=pltpu.CompilerParams(vmem_limit_bytes=20 * MIB),
        cost_estimate=pl.CostEstimate(flops=2 * rows * wide * n * heads[0].shape[1], transcendentals=0, bytes_accessed=8 * MIB),
        name="project",
    )(at, *heads, *outs, residual, gain)


CUTS = 2


def hidden_body(n, at_ref, x_ref, w_ref, down_ref, hidden_ref, low_ref, high_ref, sum_ref):
    step = pl.program_id(0)
    spread, _, deep, units = w_ref.shape
    tall = spread * deep
    which, cut = step // CUTS, step % CUTS
    more = dot(x_ref[:, pl.ds(pl.multiple_of(cut * tall, tall), tall)], w_ref[...].reshape(tall, units), 1, 0)

    @pl.when(cut == 0)
    def _():
        sum_ref[which] = more

    @pl.when(cut > 0)
    def _():
        sum_ref[which] = sum_ref[which] + more

    @pl.when(step == 2 * CUTS - 1)
    def _():
        gate = sum_ref[0]
        hidden_ref[...] = (gate / (1.0 + jnp.exp(-gate)) * sum_ref[1]).astype(bf16)
        piece = dot(hidden_ref[...], down_ref[...].reshape(-1, units), 1, 1).astype(bf16)
        half = piece.shape[0] // 2
        low_ref[...] = piece[:half]
        high_ref[...] = piece[half:]


def hidden_of(at, x, w, n):
    rows, wide = x.shape
    spread, _, deep, units = w.shape
    share = wide // n
    whole = lambda p, at: (0, 0)
    return pl.pallas_call(
        functools.partial(hidden_body, n),
        grid_spec=pltpu.PrefetchScalarGridSpec(
            num_scalar_prefetch=1,
            grid=(2 * CUTS,),
            in_specs=[
                pl.BlockSpec((rows, wide), whole),
                pl.BlockSpec((spread // CUTS, 1, deep, units), lambda p, at: (p % CUTS, p // CUTS, 0, 0)),
                pl.BlockSpec((spread // n, 1, deep, units), lambda p, at: ((at[0] + 2) % n, 2, 0, 0)),
            ],
            out_specs=(
                pl.BlockSpec((rows, units), whole),
                pl.BlockSpec((rows // 2, share), whole),
                pl.BlockSpec((rows // 2, share), whole),
            ),
            scratch_shapes=[pltpu.VMEM((2, rows, units), f32)],
        ),
        out_shape=(
            jax.ShapeDtypeStruct((rows, units), bf16),
            jax.ShapeDtypeStruct((rows // 2, share), bf16),
            jax.ShapeDtypeStruct((rows // 2, share), bf16),
        ),
        compiler_params=pltpu.CompilerParams(vmem_limit_bytes=36 * MIB, dimension_semantics=("arbitrary",)),
        cost_estimate=pl.CostEstimate(flops=4 * rows * wide * units, transcendentals=rows * units, bytes_accessed=w.size * 2),
        name="hidden",
    )(at, x, w, w)


def own_body(n, at_ref, w_ref, hidden_ref, cols_ref, out_ref, buf, sem):
    part = buf.shape[0]
    copy = pltpu.make_async_copy(w_ref.at[pl.ds(at_ref[0] * part, part), 2], buf, sem)
    copy.start()
    copy.wait()
    out_ref[...] = cols_ref[...] + 0.5 * dot(hidden_ref[...], buf[...].reshape(-1, buf.shape[2]), 1, 1)


def own_part(at, hidden, w, cols, n):
    spread, _, deep, units = w.shape
    rows, share = cols.shape
    vmem = pl.BlockSpec(memory_space=pltpu.VMEM)
    return pl.pallas_call(
        functools.partial(own_body, n),
        out_shape=jax.ShapeDtypeStruct((rows, share), f32),
        in_specs=[pl.BlockSpec(memory_space=pltpu.SMEM), pl.BlockSpec(memory_space=pltpu.HBM), vmem, vmem],
        out_specs=vmem,
        scratch_shapes=[pltpu.VMEM((spread // n, deep, units), bf16), pltpu.SemaphoreType.DMA],
        compiler_params=pltpu.CompilerParams(vmem_limit_bytes=8 * MIB),
        cost_estimate=pl.CostEstimate(flops=2 * rows * share * units, transcendentals=0, bytes_accessed=2 * share * units),
        name="own",
    )(at, w, hidden, cols)


def sides_body(n, at_ref, w_ref, hidden_ref, low_ref, high_ref, up_ref, down_ref, buf, sem):
    part = buf.shape[1]
    half = low_ref.shape[0]
    copies = []
    for i, k in enumerate((1, n - 1)):
        j = (at_ref[0] + k) % n
        copies.append(pltpu.make_async_copy(w_ref.at[pl.ds(j * part, part), 2], buf.at[i], sem.at[i]))
        copies[i].start()
    copies[0].wait()
    piece = dot(hidden_ref[...], buf[0].reshape(-1, buf.shape[3]), 1, 1)
    up_ref[:half] = (piece[:half] + low_ref[...].astype(f32)).astype(bf16)
    up_ref[half:] = piece[half:].astype(bf16)
    copies[1].wait()
    piece = dot(hidden_ref[...], buf[1].reshape(-1, buf.shape[3]), 1, 1)
    down_ref[:half] = piece[:half].astype(bf16)
    down_ref[half:] = (piece[half:] + high_ref[...].astype(f32)).astype(bf16)


def side_parts(at, hidden, w, low, high, n):
    spread, _, deep, units = w.shape
    rows = hidden.shape[0]
    share = low.shape[1]
    vmem = pl.BlockSpec(memory_space=pltpu.VMEM)
    piece = jax.ShapeDtypeStruct((rows, share), bf16)
    return pl.pallas_call(
        functools.partial(sides_body, n),
        out_shape=(piece, piece),
        in_specs=[pl.BlockSpec(memory_space=pltpu.SMEM), pl.BlockSpec(memory_space=pltpu.HBM), vmem, vmem, vmem],
        out_specs=(vmem, vmem),
        scratch_shapes=[pltpu.VMEM((2, spread // n, deep, units), bf16), pltpu.SemaphoreType.DMA((2,))],
        compiler_params=pltpu.CompilerParams(vmem_limit_bytes=12 * MIB),
        cost_estimate=pl.CostEstimate(flops=4 * rows * share * units, transcendentals=0, bytes_accessed=4 * share * units),
        name="sides",
    )(at, w, hidden, low, high)


def local(
    residual,
    queries_a,
    keys_a,
    values_a,
    queries_b,
    keys_b,
    values_b,
    mix_lambda,
    head_gain,
    out_a,
    out_b,
    norm_gain,
    w_gate,
    w_up,
    w_down,
):
    wa = queries_a.shape[1] // 2
    wb = queries_b.shape[1] // 2
    vd = values_a.shape[1]
    consts = (wa**-0.5 * log2e, wb**-0.5 * log2e)
    n = lax.axis_size("tp")
    share = residual.shape[1] // n
    at = lax.axis_index("tp").astype(jnp.int32)[None]
    at, keys_a = lax.optimization_barrier((at, keys_a))

    kv, q = pack(((keys_a, keys_b, values_a, values_b), 1), ((queries_a, queries_b), 1))
    near = [kv] + [along_z(kv, k) for k in range(1, 4)]
    queries = [q] + [along_y(q, k) for k in range(1, 4)]
    kv_far = other_core(kv)
    (oo,) = pack(((out_a, out_b), 0))
    outs = [oo] + [along_x(oo, k) for k in range(1, 4)]
    (three,) = pack(((w_gate, w_up, w_down.T), 0))
    three, near[1], near[3], *queries[1:] = lax.optimization_barrier((three, near[1], near[3], *queries[1:]))
    weights = lax.all_gather(three, "sp", axis=0, tiled=True)
    weights = in_hbm(weights.reshape(-1, 3, *w_gate.shape))

    go = functools.partial(attend, consts=consts, wa=wa, wb=wb, vd=vd)
    order = ((2, 1), (3, 0))
    pairs = [[queries[k] for k in g] for g in order]
    state = go(pairs, [kv, kv_far], None, None)
    one, three, *state = lax.optimization_barrier((near[1], near[3], *state))
    far = {1: other_core(one), 3: other_core(three)}
    state = go(pairs, [one, three], state, None)
    two, *state = lax.optimization_barrier((near[2], *state))
    last = [far[1], far[3], two, other_core(two)]
    back = {}
    for g, group in enumerate(order):
        for i, k in enumerate(group):
            done = go([[queries[k]]], last, state, (g, i, k != 0))
            if k:
                back[k] = along_y(done, -k)
            else:
                own = done
    heads = merge(own, [back[k] for k in (1, 3, 2)], mix_lambda, head_gain, consts, vd)

    everyone = [heads] + [along_x(heads, k) for k in range(1, 4)]
    normed, cols = project(at, everyone, outs, residual, norm_gain[None], share)
    hidden, low, high = hidden_of(at, normed, weights, n)
    low, high = along_x(low, 1), along_x(high, -1)
    mine = own_part(at, hidden, weights, cols, n)
    up, down = side_parts(at, hidden, weights, low, high, n)
    arrived = along_x(up, 1).astype(f32) + along_x(down, -1).astype(f32)
    return (mine + 0.5 * arrived).astype(bf16)


def solution(mesh):
    in_specs = (
        P("sp", None),
        P("sp", "tp"),
        P("sp", "tp"),
        P("sp", "tp"),
        P("sp", "tp"),
        P("sp", "tp"),
        P("sp", "tp"),
        P(None, "tp"),
        P(),
        P("tp", None),
        P("tp", None),
        P(),
        P("sp", "tp"),
        P("sp", "tp"),
        P("tp", "sp"),
    )
    out_specs = P("sp", "tp")
    return jax.shard_map(local, mesh=mesh, in_specs=in_specs, out_specs=out_specs, check_vma=False)
```

```python
import math
import functools
import jax
import jax.numpy as jnp
from jax import lax
from jax.experimental import pallas as pl
from jax.experimental.pallas import tpu as pltpu
from jax.sharding import PartitionSpec as P

eps_norm = 1e-06
head_scale = 0.8
log2e = math.log2(math.e)
f32 = jnp.float32
bf16 = jnp.bfloat16

SP = [(z, y, c) for z in range(4) for y in range(4) for c in range(2)]


def place(z, y, c):
    return (z % 4) * 8 + (y % 4) * 2 + c % 2


def along_y(x, k):
    return lax.ppermute(x, "sp", [(place(z, y, c), place(z, y + k, c)) for z, y, c in SP])


def along_z(x, k):
    return lax.ppermute(x, "sp", [(place(z, y, c), place(z + k, y, c)) for z, y, c in SP])


def other_core(x):
    return lax.ppermute(x, "sp", [(place(z, y, c), place(z, y, c + 1)) for z, y, c in SP])


def along_x(x, k):
    return lax.ppermute(x, "tp", [(i, (i + k) % 4) for i in range(4)])


def dot(a, b, ca, cb):
    return lax.dot_general(a, b, (((ca,), (cb,)), ((), ())), preferred_element_type=f32)


def pack_body(layout, *refs):
    n = sum(len(parts) for parts in layout)
    ins, outs, sem = refs[:n], refs[n:-1], refs[-1]
    copies, i = [], 0
    for out, parts in zip(outs, layout):
        for corner in parts:
            part = tuple(pl.ds(c, d) for c, d in zip(corner, ins[i].shape))
            copies.append(pltpu.make_async_copy(ins[i], out.at[part], sem.at[i]))
            i += 1
    for c in copies:
        c.start()
    for c in copies:
        c.wait()


def in_hbm(x):
    return pltpu.with_memory_space_constraint(x, pltpu.HBM)


def pack(*sides, far=False, fixed=True):
    layout, shapes = [], []
    for arrays, axis in sides:
        at, corners = 0, []
        for a in arrays:
            corners.append((at, 0) if axis == 0 else (0, at))
            at += a.shape[axis]
        other = arrays[0].shape[1 - axis]
        layout.append(corners)
        shapes.append(jax.ShapeDtypeStruct((at, other) if axis == 0 else (other, at), arrays[0].dtype))
    flat = [in_hbm(a) if fixed else a for arrays, _ in sides for a in arrays]
    return pl.pallas_call(
        functools.partial(pack_body, layout),
        out_shape=tuple(shapes),
        in_specs=[pl.BlockSpec(memory_space=pltpu.HBM)] * len(flat),
        out_specs=tuple(pl.BlockSpec(memory_space=pl.ANY if far else pltpu.VMEM) for _ in shapes),
        scratch_shapes=[pltpu.SemaphoreType.DMA((len(flat),))],
        compiler_params=pltpu.CompilerParams(vmem_limit_bytes=8 * MIB),
        name="pack",
    )(*flat)


AHEAD = 3
MIB = 1024 * 1024


def attend_body(groups, m, nk, carry, pick, consts, rows, wa, wb, vd, *refs):
    nq = groups * m
    q_refs, refs = refs[:nq], refs[nq:]
    kv_refs, refs = refs[:nk], refs[nk:]
    if carry:
        acc_in, ml_in, refs = refs[0], refs[1], refs[2:]
    send = pick is not None and pick[2]
    outs = 1 if send else 2
    q_buf, kv_buf, pad_buf, q_sem, kv_sem, acc_sem = refs[outs : outs + 6]
    turned = None
    rest = refs[outs + 6 :]
    if groups > 1:
        turned, rest = rest[0], rest[1:]
    if send:
        o_ref = refs[0]
        acc_ref, ml_ref = rest
    else:
        acc_ref, ml_ref = refs[:2]
    q_copies = [
        pltpu.make_async_copy(q_refs[i], q_buf.at[i // m, pl.ds((i % m) * rows, rows)], q_sem.at[i]) for i in range(nq)
    ]
    kv_copies = [
        pltpu.make_async_copy(kv_refs[i], kv_buf.at[pl.ds(i * rows, rows)], kv_sem.at[i]) for i in range(nk)
    ]
    if carry:
        if pick is not None:
            lanes = pl.ds(pick[1] * rows, rows)
            acc_in = acc_in.at[pl.ds(pick[0], 1), :, lanes]
            ml_in = ml_in.at[pl.ds(pick[0], 1), :, lanes]
        acc_copies = [
            pltpu.make_async_copy(acc_in, acc_ref, acc_sem.at[0]),
            pltpu.make_async_copy(ml_in, ml_ref, acc_sem.at[1]),
        ]
    else:
        acc_copies = []
    per = 2 if m > 1 else 1
    for c in q_copies + kv_copies[:per] + acc_copies + kv_copies[per:]:
        c.start()
    if not carry:
        acc_ref[...] = jnp.zeros_like(acc_ref)
        ml_ref[:, 0:8, :] = jnp.full((groups, 8, m * rows), -jnp.inf, f32)
        ml_ref[:, 8:16, :] = jnp.zeros((groups, 8, m * rows), f32)
    for c in q_copies:
        c.wait()
    for g in range(groups):
        qa = q_buf[g, :, 0 : 2 * wa]
        col = lax.broadcasted_iota(jnp.int32, qa.shape, 1)
        zero = jnp.zeros_like(qa)
        pad_buf[g, :, 0 : 2 * wa] = jnp.where(col < wa, qa, zero)
        pad_buf[g, :, 2 * wa :] = jnp.where(col >= wa, qa, zero)
    for c in acc_copies:
        c.wait()
    steps = nk // per
    tall = per * rows
    wide = m * rows
    lane = 256 if wide % 256 == 0 else wide
    items = [(h, j) for h in range(wide // lane) for j in range(4)]

    def step(t, _):
        qi = t // steps
        ci = t % steps
        keys = pl.ds(pl.multiple_of(ci * tall, tall), tall)

        @pl.when(qi == 0)
        def _():
            for b in range(per):
                i = ci * per + b
                pltpu.make_async_copy(kv_refs[0], kv_buf.at[pl.ds(i * rows, rows)], kv_sem.at[i]).wait()
            if turned is not None:
                first = lax.broadcasted_iota(jnp.int32, (16, tall), 0) == 0
                for g in range(2):
                    at = 2 * wa + 2 * wb + g * vd
                    turned[ci, g, 0:vd, :] = kv_buf[keys, at : at + vd].T
                    turned[ci, g, vd : vd + 16, :] = jnp.where(first, 1.0, 0.0).astype(bf16)

        def score(h, j):
            lanes = slice(h * lane, (h + 1) * lane)
            if j < 2:
                return dot(kv_buf[keys, 0 : 2 * wa], pad_buf[qi, lanes, j * 2 * wa : (j + 1) * 2 * wa], 1, 1)
            at = 2 * wa + (j - 2) * wb
            return dot(kv_buf[keys, at : at + wb], q_buf[qi, lanes, at : at + wb], 1, 1)

        ready = [score(*item) for item in items[:AHEAD]]
        for n, (h, j) in enumerate(items):
            if n + AHEAD < len(items):
                ready.append(score(*items[n + AHEAD]))
            s = ready.pop(0)
            lanes = slice(h * lane, (h + 1) * lane)
            c = consts[j // 2]
            old = ml_ref[qi, j : j + 1, lanes]
            top = jnp.maximum(old, jnp.max(s, axis=0, keepdims=True))
            w = jnp.exp2((s - top) * c)
            decay = jnp.exp2((old - top) * c)
            ml_ref[qi, j : j + 1, lanes] = top
            if turned is not None:
                more = dot(turned[ci, j // 2], w.astype(bf16), 1, 0)
                total = more[vd : vd + 1]
                more = more[0:vd]
            else:
                total = jnp.sum(w, axis=0, keepdims=True)
                at = 2 * wa + 2 * wb + (j // 2) * vd
                more = dot(kv_buf[keys, at : at + vd], w.astype(bf16), 0, 0)
            ml_ref[qi, j + 8 : j + 9, lanes] = ml_ref[qi, j + 8 : j + 9, lanes] * decay + total
            part = slice(j * vd, (j + 1) * vd)
            acc_ref[qi, part, lanes] = acc_ref[qi, part, lanes] * decay + more
        return 0

    lax.fori_loop(0, groups * steps, step, 0)
    if send:
        for j in range(4):
            part = slice(j * vd, (j + 1) * vd)
            inverse = 1.0 / ml_ref[0, j + 8 : j + 9, :]
            o_ref[part, :] = (acc_ref[0, part, :] * inverse).astype(bf16)
        level = level_of(ml_ref, consts)
        high = level.astype(bf16).astype(f32)
        mid = (level - high).astype(bf16).astype(f32)
        low = level - high - mid
        o_ref[4 * vd :, :] = jnp.concatenate([high, mid, low, jnp.zeros_like(low)], axis=0).astype(bf16)


def level_of(ml_ref, consts):
    row = lax.broadcasted_iota(jnp.int32, (8, ml_ref.shape[2]), 0)
    used = row < 4
    top = jnp.where(used, ml_ref[0, 0:8, :], 0.0)
    total = jnp.where(used, ml_ref[0, 8:16, :], 1.0)
    return top * jnp.where(row < 2, consts[0], consts[1]) + jnp.log2(total)


def attend(queries, blocks, state, pick, consts, wa, wb, vd):
    groups, m = len(queries), len(queries[0])
    flat = [q for g in queries for q in g]
    nq, nk = len(flat), len(blocks)
    rows = flat[0].shape[0]
    wide = flat[0].shape[1]
    cols = blocks[0].shape[1]
    anywhere = pl.BlockSpec(memory_space=pl.ANY)
    vmem = pl.BlockSpec(memory_space=pltpu.VMEM)
    acc_shape = (groups, 4 * vd, m * rows)
    ml_shape = (groups, 16, m * rows)
    scratch = [
        pltpu.VMEM((groups, m * rows, wide), bf16),
        pltpu.VMEM((nk * rows, cols), bf16),
        pltpu.VMEM((groups, m * rows, 4 * wa), bf16),
        pltpu.SemaphoreType.DMA((nq,)),
        pltpu.SemaphoreType.DMA((nk,)),
        pltpu.SemaphoreType.DMA((2,)),
    ]
    if groups > 1:
        per = 2 if m > 1 else 1
        scratch.append(pltpu.VMEM((nk // per, 2, vd + 16, per * rows), bf16))
    if pick is not None and pick[2]:
        out_shape = jax.ShapeDtypeStruct((4 * vd + 32, rows), bf16)
        out_specs = vmem
        scratch += [pltpu.VMEM(acc_shape, f32), pltpu.VMEM(ml_shape, f32)]
    else:
        out_shape = (jax.ShapeDtypeStruct(acc_shape, f32), jax.ShapeDtypeStruct(ml_shape, f32))
        out_specs = (vmem, vmem)
    work = nq * nk * rows * rows
    return pl.pallas_call(
        functools.partial(attend_body, groups, m, nk, state is not None, pick, consts, rows, wa, wb, vd),
        out_shape=out_shape,
        in_specs=[anywhere] * (nq + nk + (0 if state is None else 2)),
        out_specs=out_specs,
        scratch_shapes=scratch,
        compiler_params=pltpu.CompilerParams(vmem_limit_bytes=16 * MIB),
        cost_estimate=pl.CostEstimate(flops=work * 4 * 4 * vd, transcendentals=4 * work, bytes_accessed=nk * rows * cols * 2),
        name="attend",
    )(*flat, *blocks, *(state or ()))


def merge_body(consts, vd, lam_ref, gain_ref, acc_ref, ml_ref, *refs):
    others, out_ref = refs[:-1], refs[-1]
    levels = [level_of(ml_ref, consts)]
    for o in others:
        stats = o[4 * vd :, :].astype(f32)
        levels.append(stats[0:8] + stats[8:16] + stats[16:24])
    top = functools.reduce(jnp.maximum, levels)
    shares = [jnp.exp2(v - top) for v in levels]
    inverse = 1.0 / functools.reduce(jnp.add, shares)
    shares = [v * inverse for v in shares]
    for g in range(2):
        ratio = []
        for j in (2 * g, 2 * g + 1):
            part = slice(j * vd, (j + 1) * vd)
            value = acc_ref[0, part, :] * (shares[0][j : j + 1] / ml_ref[0, j + 8 : j + 9, :])
            for o, share in zip(others, shares[1:]):
                value = value + o[part, :].astype(f32) * share[j : j + 1]
            ratio.append(value)
        mixed = ratio[0] - lam_ref[0:1, g : g + 1] * ratio[1]
        scale = lax.rsqrt(jnp.mean(mixed * mixed, axis=0, keepdims=True) + eps_norm)
        normed = (mixed * scale).T * gain_ref[g : g + 1, :] * head_scale
        out_ref[:, g * vd : (g + 1) * vd] = normed.astype(bf16)


def merge(state, others, lam, gain, consts, vd):
    rows = state[1].shape[-1]
    vmem = pl.BlockSpec(memory_space=pltpu.VMEM)
    return pl.pallas_call(
        functools.partial(merge_body, consts, vd),
        out_shape=jax.ShapeDtypeStruct((rows, 2 * vd), bf16),
        in_specs=[vmem] * (4 + len(others)),
        out_specs=vmem,
        compiler_params=pltpu.CompilerParams(vmem_limit_bytes=12 * MIB),
        name="merge",
    )(lam.T, gain, *state, *others)


def project_body(n, share, *refs):
    place_ref, heads, outs = refs[0], refs[1 : 1 + n], refs[1 + n : 1 + 2 * n]
    residual_ref, gain_ref, normed_ref, cols_ref, summed_ref = refs[1 + 2 * n :]
    some = residual_ref.shape[0] // 2

    def part(i, _):
        rows = pl.ds(pl.multiple_of(i * some, some), some)
        total = residual_ref[rows, :].astype(f32)
        for h, o in zip(heads, outs):
            total = total + dot(h[rows, :], o[...], 1, 0)
        summed_ref[rows, :] = total
        inverse = lax.rsqrt(jnp.mean(total * total, axis=-1, keepdims=True) + eps_norm)
        normed_ref[rows, :] = (summed_ref[rows, :] * inverse * gain_ref[...]).astype(bf16)
        return 0

    lax.fori_loop(0, 2, part, 0)
    cols_ref[...] = summed_ref[:, pl.ds(pl.multiple_of(place_ref[0] * share, share), share)]


def project(at, heads, outs, residual, gain, share):
    n = len(heads)
    rows, wide = residual.shape
    vmem = pl.BlockSpec(memory_space=pltpu.VMEM)
    smem = pl.BlockSpec(memory_space=pltpu.SMEM)
    return pl.pallas_call(
        functools.partial(project_body, n, share),
        out_shape=(jax.ShapeDtypeStruct((rows, wide), bf16), jax.ShapeDtypeStruct((rows, share), f32)),
        in_specs=[smem] + [vmem] * (2 * n + 2),
        out_specs=(vmem, vmem),
        scratch_shapes=[pltpu.VMEM((rows, wide), f32)],
        compiler_params=pltpu.CompilerParams(vmem_limit_bytes=20 * MIB),
        cost_estimate=pl.CostEstimate(flops=2 * rows * wide * n * heads[0].shape[1], transcendentals=0, bytes_accessed=8 * MIB),
        name="project",
    )(at, *heads, *outs, residual, gain)


CUTS = 4


def fetch(place_ref, k, n, arrays, buf, sem):
    spot = place_ref[1]
    y_here, z_here, core = (spot // 2) % 4, spot // 8, spot % 2
    source = (z_here + n - (place_ref[0] + k) % n) % n
    for i in range(n):

        @pl.when(source == i)
        def _():
            def one(y, _):
                to = ((y_here + 4 - y) % 4) * 2
                for c in range(2):
                    pltpu.make_async_copy(arrays[c * n + i].at[y], buf.at[to + (core + c) % 2], sem).start()
                return 0

            lax.fori_loop(0, 4, one, 0)


def fetched(buf, sem):
    pltpu.make_async_copy(buf, buf, sem).wait()


def hidden_body(n, place_ref, x_ref, w_ref, *refs):
    arrays, refs = refs[: 2 * n], refs[2 * n :]
    hidden_ref, low_ref, high_ref, sum_ref, buf, sem = refs
    step = pl.program_id(0)
    spread, _, deep, units = w_ref.shape
    tall = spread * deep
    which, cut = step // CUTS, step % CUTS

    @pl.when(step == 0)
    def _():
        fetch(place_ref, 2, n, arrays, buf, sem)

    more = dot(x_ref[:, pl.ds(pl.multiple_of(cut * tall, tall), tall)], w_ref[...].reshape(tall, units), 1, 0)

    @pl.when(cut == 0)
    def _():
        sum_ref[which] = more

    @pl.when(cut > 0)
    def _():
        sum_ref[which] = sum_ref[which] + more

    @pl.when(step == 2 * CUTS - 1)
    def _():
        gate = sum_ref[0]
        hidden_ref[...] = (gate / (1.0 + jnp.exp(-gate)) * sum_ref[1]).astype(bf16)
        fetched(buf, sem)
        piece = dot(hidden_ref[...], buf[...].reshape(-1, units), 1, 1).astype(bf16)
        half = piece.shape[0] // 2
        low_ref[...] = piece[:half]
        high_ref[...] = piece[half:]


def hidden_of(place, x, w, downs, n):
    rows, wide = x.shape
    spread, _, deep, units = w.shape
    share = wide // n
    whole = lambda p, place: (0, 0)
    return pl.pallas_call(
        functools.partial(hidden_body, n),
        grid_spec=pltpu.PrefetchScalarGridSpec(
            num_scalar_prefetch=1,
            grid=(2 * CUTS,),
            in_specs=[
                pl.BlockSpec((rows, wide), whole),
                pl.BlockSpec((spread // CUTS, 1, deep, units), lambda p, place: (p % CUTS, p // CUTS, 0, 0)),
            ]
            + [pl.BlockSpec(memory_space=pltpu.HBM)] * (2 * n),
            out_specs=(
                pl.BlockSpec((rows, units), whole),
                pl.BlockSpec((rows // 2, share), whole),
                pl.BlockSpec((rows // 2, share), whole),
            ),
            scratch_shapes=[
                pltpu.VMEM((2, rows, units), f32),
                pltpu.VMEM((8, deep, units), bf16),
                pltpu.SemaphoreType.DMA,
            ],
        ),
        out_shape=(
            jax.ShapeDtypeStruct((rows, units), bf16),
            jax.ShapeDtypeStruct((rows // 2, share), bf16),
            jax.ShapeDtypeStruct((rows // 2, share), bf16),
        ),
        compiler_params=pltpu.CompilerParams(vmem_limit_bytes=30 * MIB, dimension_semantics=("arbitrary",)),
        cost_estimate=pl.CostEstimate(flops=4 * rows * wide * units, transcendentals=rows * units, bytes_accessed=w.size * 2),
        name="hidden",
    )(place, x, w, *downs)


def own_body(n, place_ref, hidden_ref, cols_ref, *refs):
    arrays = refs[: 2 * n]
    out_ref, buf, sem = refs[2 * n :]
    fetch(place_ref, 0, n, arrays, buf, sem)
    fetched(buf, sem)
    out_ref[...] = cols_ref[...] + 0.5 * dot(hidden_ref[...], buf[...].reshape(-1, buf.shape[2]), 1, 1)


def own_part(place, hidden, downs, cols, n):
    rows, share = cols.shape
    _, deep, units = downs[0].shape
    vmem = pl.BlockSpec(memory_space=pltpu.VMEM)
    return pl.pallas_call(
        functools.partial(own_body, n),
        out_shape=jax.ShapeDtypeStruct((rows, share), f32),
        in_specs=[pl.BlockSpec(memory_space=pltpu.SMEM), vmem, vmem] + [pl.BlockSpec(memory_space=pltpu.HBM)] * (2 * n),
        out_specs=vmem,
        scratch_shapes=[pltpu.VMEM((8, deep, units), bf16), pltpu.SemaphoreType.DMA],
        compiler_params=pltpu.CompilerParams(vmem_limit_bytes=8 * MIB),
        cost_estimate=pl.CostEstimate(flops=2 * rows * share * units, transcendentals=0, bytes_accessed=2 * share * units),
        name="own",
    )(place, hidden, cols, *downs)


def sides_body(n, place_ref, hidden_ref, low_ref, high_ref, *refs):
    arrays = refs[: 2 * n]
    up_ref, down_ref, buf, sem = refs[2 * n :]
    half = low_ref.shape[0]
    fetch(place_ref, 1, n, arrays, buf.at[0], sem.at[0])
    fetch(place_ref, n - 1, n, arrays, buf.at[1], sem.at[1])
    fetched(buf.at[0], sem.at[0])
    piece = dot(hidden_ref[...], buf[0].reshape(-1, buf.shape[3]), 1, 1)
    up_ref[:half] = (piece[:half] + low_ref[...].astype(f32)).astype(bf16)
    up_ref[half:] = piece[half:].astype(bf16)
    fetched(buf.at[1], sem.at[1])
    piece = dot(hidden_ref[...], buf[1].reshape(-1, buf.shape[3]), 1, 1)
    down_ref[:half] = piece[:half].astype(bf16)
    down_ref[half:] = (piece[half:] + high_ref[...].astype(f32)).astype(bf16)


def side_parts(place, hidden, downs, low, high, n):
    _, deep, units = downs[0].shape
    rows = hidden.shape[0]
    share = low.shape[1]
    vmem = pl.BlockSpec(memory_space=pltpu.VMEM)
    piece = jax.ShapeDtypeStruct((rows, share), bf16)
    return pl.pallas_call(
        functools.partial(sides_body, n),
        out_shape=(piece, piece),
        in_specs=[pl.BlockSpec(memory_space=pltpu.SMEM), vmem, vmem, vmem]
        + [pl.BlockSpec(memory_space=pltpu.HBM)] * (2 * n),
        out_specs=(vmem, vmem),
        scratch_shapes=[pltpu.VMEM((2, 8, deep, units), bf16), pltpu.SemaphoreType.DMA((2,))],
        compiler_params=pltpu.CompilerParams(vmem_limit_bytes=12 * MIB),
        cost_estimate=pl.CostEstimate(flops=4 * rows * share * units, transcendentals=0, bytes_accessed=4 * share * units),
        name="sides",
    )(place, hidden, low, high, *downs)


def local(
    residual,
    queries_a,
    keys_a,
    values_a,
    queries_b,
    keys_b,
    values_b,
    mix_lambda,
    head_gain,
    out_a,
    out_b,
    norm_gain,
    w_gate,
    w_up,
    w_down,
):
    wa = queries_a.shape[1] // 2
    wb = queries_b.shape[1] // 2
    vd = values_a.shape[1]
    consts = (wa**-0.5 * log2e, wb**-0.5 * log2e)
    n = lax.axis_size("tp")
    share = residual.shape[1] // n
    where = jnp.stack([lax.axis_index("tp"), lax.axis_index("sp")]).astype(jnp.int32)
    where, keys_a = lax.optimization_barrier((where, keys_a))

    kv, q = pack(((keys_a, keys_b, values_a, values_b), 1), ((queries_a, queries_b), 1))
    near = [kv, along_z(kv, 1), None, along_z(kv, 3)]
    queries = [q] + [along_y(q, k) for k in range(1, 4)]
    kv_far = other_core(kv)
    down = w_down.T
    downs = [down] + [along_y(down, k) for k in range(1, 4)]
    (oo,) = pack(((out_a, out_b), 0))
    outs = [oo] + [along_x(oo, k) for k in range(1, 4)]
    (two,) = pack(((w_gate, w_up), 0), far=True)
    two, near[1], near[3], *queries[1:] = lax.optimization_barrier((two, near[1], near[3], *queries[1:]))
    kv, queries[1] = lax.optimization_barrier((kv, queries[1]))
    near[2] = along_z(kv, 2)
    weights = lax.all_gather(two, "sp", axis=0, tiled=True)
    weights = in_hbm(weights.reshape(-1, 2, *w_gate.shape))

    go = functools.partial(attend, consts=consts, wa=wa, wb=wb, vd=vd)
    order = ((2, 1), (3, 0))
    pairs = [[queries[k] for k in g] for g in order]
    state = go(pairs, [kv, kv_far], None, None)
    one, three, *state = lax.optimization_barrier((near[1], near[3], *state))
    *downs, kept = lax.optimization_barrier((*downs, state[1]))
    state[1] = kept
    (column,) = pack((downs, 0), fixed=False)
    columns = [column] + [along_z(column, k) for k in range(1, 4)]
    far = {1: other_core(one), 3: other_core(three)}
    state = go(pairs, [one, three], state, None)
    two, *state = lax.optimization_barrier((near[2], *state))
    last = [far[1], far[3], two, other_core(two)]
    back = {}
    for g, group in enumerate(order):
        for i, k in enumerate(group):
            done = go([[queries[k]]], last, state, (g, i, k != 0))
            if k:
                back[k] = along_y(done, -k)
            else:
                own = done
    columns, own = lax.optimization_barrier((columns, own))
    columns = columns + [other_core(c) for c in columns]
    columns = [in_hbm(c.reshape(4, -1, c.shape[1])) for c in columns]
    heads = merge(own, [back[k] for k in (1, 3, 2)], mix_lambda, head_gain, consts, vd)

    everyone = [heads] + [along_x(heads, k) for k in range(1, 4)]
    normed, cols = project(where, everyone, outs, residual, norm_gain[None], share)
    hidden, low, high = hidden_of(where, normed, weights, columns, n)
    low, high = along_x(low, 1), along_x(high, -1)
    mine = own_part(where, hidden, columns, cols, n)
    up, down = side_parts(where, hidden, columns, low, high, n)
    arrived = along_x(up, 1).astype(f32) + along_x(down, -1).astype(f32)
    return (mine + 0.5 * arrived).astype(bf16)


def solution(mesh):
    in_specs = (
        P("sp", None),
        P("sp", "tp"),
        P("sp", "tp"),
        P("sp", "tp"),
        P("sp", "tp"),
        P("sp", "tp"),
        P("sp", "tp"),
        P(None, "tp"),
        P(),
        P("tp", None),
        P("tp", None),
        P(),
        P("sp", "tp"),
        P("sp", "tp"),
        P("tp", "sp"),
    )
    out_specs = P("sp", "tp")

    return jax.shard_map(local, mesh=mesh, in_specs=in_specs, out_specs=out_specs, check_vma=False)
```

```python
import math
import functools
import jax
import jax.numpy as jnp
from jax import lax
from jax.experimental import pallas as pl
from jax.experimental.pallas import tpu as pltpu
from jax.sharding import PartitionSpec as P

eps_norm = 1e-06
head_scale = 0.8
log2e = math.log2(math.e)
f32 = jnp.float32
bf16 = jnp.bfloat16

SP = [(z, y, c) for z in range(4) for y in range(4) for c in range(2)]


def place(z, y, c):
    return (z % 4) * 8 + (y % 4) * 2 + c % 2


def along_y(x, k):
    return lax.ppermute(x, "sp", [(place(z, y, c), place(z, y + k, c)) for z, y, c in SP])


def along_z(x, k):
    return lax.ppermute(x, "sp", [(place(z, y, c), place(z + k, y, c)) for z, y, c in SP])


def other_core(x):
    return lax.ppermute(x, "sp", [(place(z, y, c), place(z, y, c + 1)) for z, y, c in SP])


def along_x(x, k):
    return lax.ppermute(x, "tp", [(i, (i + k) % 4) for i in range(4)])


def dot(a, b, ca, cb):
    return lax.dot_general(a, b, (((ca,), (cb,)), ((), ())), preferred_element_type=f32)


def pack_body(layout, *refs):
    n = sum(len(parts) for parts in layout)
    ins, outs, sem = refs[:n], refs[n:-1], refs[-1]
    copies, i = [], 0
    for out, parts in zip(outs, layout):
        for corner in parts:
            part = tuple(pl.ds(c, d) for c, d in zip(corner, ins[i].shape))
            copies.append(pltpu.make_async_copy(ins[i], out.at[part], sem.at[i]))
            i += 1
    for c in copies:
        c.start()
    for c in copies:
        c.wait()


def in_hbm(x):
    return pltpu.with_memory_space_constraint(x, pltpu.HBM)


def pack(*sides):
    layout, shapes = [], []
    for arrays, axis in sides:
        at, corners = 0, []
        for a in arrays:
            corners.append((at, 0) if axis == 0 else (0, at))
            at += a.shape[axis]
        other = arrays[0].shape[1 - axis]
        layout.append(corners)
        shapes.append(jax.ShapeDtypeStruct((at, other) if axis == 0 else (other, at), arrays[0].dtype))
    flat = [in_hbm(a) for arrays, _ in sides for a in arrays]
    return pl.pallas_call(
        functools.partial(pack_body, layout),
        out_shape=tuple(shapes),
        in_specs=[pl.BlockSpec(memory_space=pltpu.HBM)] * len(flat),
        out_specs=tuple(pl.BlockSpec(memory_space=pltpu.VMEM) for _ in shapes),
        scratch_shapes=[pltpu.SemaphoreType.DMA((len(flat),))],
        compiler_params=pltpu.CompilerParams(vmem_limit_bytes=8 * MIB),
        name="pack",
    )(*flat)


PER = 2
AHEAD = 3
MIB = 1024 * 1024


def attend_body(groups, m, nk, carry, pick, consts, rows, wa, wb, vd, *refs):
    nq = groups * m
    q_refs, refs = refs[:nq], refs[nq:]
    kv_refs, refs = refs[:nk], refs[nk:]
    if carry:
        acc_in, ml_in, refs = refs[0], refs[1], refs[2:]
    send = pick is not None and pick[2]
    outs = m if send else 2
    q_buf, kv_buf, pad_buf, q_sem, kv_sem, acc_sem = refs[outs : outs + 6]
    turned = None
    rest = refs[outs + 6 :]
    if groups > 1:
        turned, rest = rest[0], rest[1:]
    if send:
        o_refs = refs[:m]
        acc_ref, ml_ref = rest
    else:
        acc_ref, ml_ref = refs[:2]
    q_copies = [
        pltpu.make_async_copy(q_refs[i], q_buf.at[i // m, pl.ds((i % m) * rows, rows)], q_sem.at[i]) for i in range(nq)
    ]
    kv_copies = [
        pltpu.make_async_copy(kv_refs[i], kv_buf.at[pl.ds(i * rows, rows)], kv_sem.at[i]) for i in range(nk)
    ]
    if carry:
        if pick is not None:
            lanes = pl.ds(pick[1] * rows, m * rows)
            acc_in = acc_in.at[pl.ds(pick[0], 1), :, lanes]
            ml_in = ml_in.at[pl.ds(pick[0], 1), :, lanes]
        acc_copies = [
            pltpu.make_async_copy(acc_in, acc_ref, acc_sem.at[0]),
            pltpu.make_async_copy(ml_in, ml_ref, acc_sem.at[1]),
        ]
    else:
        acc_copies = []
    per = min(PER, nk)
    for c in q_copies + kv_copies[:per] + acc_copies + kv_copies[per:]:
        c.start()
    if not carry:
        acc_ref[...] = jnp.zeros_like(acc_ref)
        ml_ref[:, 0:8, :] = jnp.full((groups, 8, m * rows), -jnp.inf, f32)
        ml_ref[:, 8:16, :] = jnp.zeros((groups, 8, m * rows), f32)
    for c in q_copies:
        c.wait()
    for g in range(groups):
        qa = q_buf[g, :, 0 : 2 * wa]
        col = lax.broadcasted_iota(jnp.int32, qa.shape, 1)
        zero = jnp.zeros_like(qa)
        pad_buf[g, :, 0 : 2 * wa] = jnp.where(col < wa, qa, zero)
        pad_buf[g, :, 2 * wa :] = jnp.where(col >= wa, qa, zero)
    for c in acc_copies:
        c.wait()
    steps = nk // per
    tall = per * rows
    wide = m * rows
    lane = 256 if wide % 256 == 0 else wide
    items = [(h, j) for h in range(wide // lane) for j in range(4)]

    def step(t, _):
        qi = t // steps
        ci = t % steps
        keys = pl.ds(pl.multiple_of(ci * tall, tall), tall)

        @pl.when(qi == 0)
        def _():
            for b in range(per):
                i = ci * per + b
                pltpu.make_async_copy(kv_refs[0], kv_buf.at[pl.ds(i * rows, rows)], kv_sem.at[i]).wait()
            if turned is not None:
                first = lax.broadcasted_iota(jnp.int32, (16, tall), 0) == 0
                for g in range(2):
                    at = 2 * wa + 2 * wb + g * vd
                    turned[ci, g, 0:vd, :] = kv_buf[keys, at : at + vd].T
                    turned[ci, g, vd : vd + 16, :] = jnp.where(first, 1.0, 0.0).astype(bf16)

        def score(h, j):
            lanes = slice(h * lane, (h + 1) * lane)
            if j < 2:
                return dot(kv_buf[keys, 0 : 2 * wa], pad_buf[qi, lanes, j * 2 * wa : (j + 1) * 2 * wa], 1, 1)
            at = 2 * wa + (j - 2) * wb
            return dot(kv_buf[keys, at : at + wb], q_buf[qi, lanes, at : at + wb], 1, 1)

        ready = [score(*item) for item in items[:AHEAD]]
        for n, (h, j) in enumerate(items):
            if n + AHEAD < len(items):
                ready.append(score(*items[n + AHEAD]))
            s = ready.pop(0)
            lanes = slice(h * lane, (h + 1) * lane)
            c = consts[j // 2]
            old = ml_ref[qi, j : j + 1, lanes]
            top = jnp.maximum(old, jnp.max(s, axis=0, keepdims=True))
            w = jnp.exp2((s - top) * c)
            decay = jnp.exp2((old - top) * c)
            ml_ref[qi, j : j + 1, lanes] = top
            if turned is not None:
                more = dot(turned[ci, j // 2], w.astype(bf16), 1, 0)
                total = more[vd : vd + 1]
                more = more[0:vd]
            else:
                total = jnp.sum(w, axis=0, keepdims=True)
                at = 2 * wa + 2 * wb + (j // 2) * vd
                more = dot(kv_buf[keys, at : at + vd], w.astype(bf16), 0, 0)
            ml_ref[qi, j + 8 : j + 9, lanes] = ml_ref[qi, j + 8 : j + 9, lanes] * decay + total
            part = slice(j * vd, (j + 1) * vd)
            acc_ref[qi, part, lanes] = acc_ref[qi, part, lanes] * decay + more
        return 0

    lax.fori_loop(0, groups * steps, step, 0)
    if send:
        level = level_of(ml_ref, consts)
        high = level.astype(bf16).astype(f32)
        mid = (level - high).astype(bf16).astype(f32)
        low = level - high - mid
        stats = jnp.concatenate([high, mid, low, jnp.zeros_like(low)], axis=0).astype(bf16)
        for i, o_ref in enumerate(o_refs):
            lanes = slice(i * rows, (i + 1) * rows)
            for j in range(4):
                part = slice(j * vd, (j + 1) * vd)
                inverse = 1.0 / ml_ref[0, j + 8 : j + 9, lanes]
                o_ref[part, :] = (acc_ref[0, part, lanes] * inverse).astype(bf16)
            o_ref[4 * vd :, :] = stats[:, lanes]


def level_of(ml_ref, consts):
    row = lax.broadcasted_iota(jnp.int32, (8, ml_ref.shape[2]), 0)
    used = row < 4
    top = jnp.where(used, ml_ref[0, 0:8, :], 0.0)
    total = jnp.where(used, ml_ref[0, 8:16, :], 1.0)
    return top * jnp.where(row < 2, consts[0], consts[1]) + jnp.log2(total)


def attend(queries, blocks, state, pick, consts, wa, wb, vd):
    groups, m = len(queries), len(queries[0])
    flat = [q for g in queries for q in g]
    nq, nk = len(flat), len(blocks)
    rows = flat[0].shape[0]
    wide = flat[0].shape[1]
    cols = blocks[0].shape[1]
    anywhere = pl.BlockSpec(memory_space=pl.ANY)
    vmem = pl.BlockSpec(memory_space=pltpu.VMEM)
    acc_shape = (groups, 4 * vd, m * rows)
    ml_shape = (groups, 16, m * rows)
    scratch = [
        pltpu.VMEM((groups, m * rows, wide), bf16),
        pltpu.VMEM((nk * rows, cols), bf16),
        pltpu.VMEM((groups, m * rows, 4 * wa), bf16),
        pltpu.SemaphoreType.DMA((nq,)),
        pltpu.SemaphoreType.DMA((nk,)),
        pltpu.SemaphoreType.DMA((2,)),
    ]
    if groups > 1:
        per = min(PER, nk)
        scratch.append(pltpu.VMEM((nk // per, 2, vd + 16, per * rows), bf16))
    if pick is not None and pick[2]:
        out_shape = (jax.ShapeDtypeStruct((4 * vd + 32, rows), bf16),) * m
        out_specs = (vmem,) * m
        scratch += [pltpu.VMEM(acc_shape, f32), pltpu.VMEM(ml_shape, f32)]
    else:
        out_shape = (jax.ShapeDtypeStruct(acc_shape, f32), jax.ShapeDtypeStruct(ml_shape, f32))
        out_specs = (vmem, vmem)
    work = nq * nk * rows * rows
    return pl.pallas_call(
        functools.partial(attend_body, groups, m, nk, state is not None, pick, consts, rows, wa, wb, vd),
        out_shape=out_shape,
        in_specs=[anywhere] * (nq + nk + (0 if state is None else 2)),
        out_specs=out_specs,
        scratch_shapes=scratch,
        compiler_params=pltpu.CompilerParams(vmem_limit_bytes=16 * MIB),
        cost_estimate=pl.CostEstimate(flops=work * 4 * 4 * vd, transcendentals=4 * work, bytes_accessed=nk * rows * cols * 2),
        name="attend",
    )(*flat, *blocks, *(state or ()))


def merge_body(consts, vd, lam_ref, gain_ref, acc_ref, ml_ref, *refs):
    others, out_ref = refs[:-1], refs[-1]
    levels = [level_of(ml_ref, consts)]
    for o in others:
        stats = o[4 * vd :, :].astype(f32)
        levels.append(stats[0:8] + stats[8:16] + stats[16:24])
    top = functools.reduce(jnp.maximum, levels)
    shares = [jnp.exp2(v - top) for v in levels]
    inverse = 1.0 / functools.reduce(jnp.add, shares)
    shares = [v * inverse for v in shares]
    for g in range(2):
        ratio = []
        for j in (2 * g, 2 * g + 1):
            part = slice(j * vd, (j + 1) * vd)
            value = acc_ref[0, part, :] * (shares[0][j : j + 1] / ml_ref[0, j + 8 : j + 9, :])
            for o, share in zip(others, shares[1:]):
                value = value + o[part, :].astype(f32) * share[j : j + 1]
            ratio.append(value)
        mixed = ratio[0] - lam_ref[0:1, g : g + 1] * ratio[1]
        scale = lax.rsqrt(jnp.mean(mixed * mixed, axis=0, keepdims=True) + eps_norm)
        normed = (mixed * scale).T * gain_ref[g : g + 1, :] * head_scale
        out_ref[:, g * vd : (g + 1) * vd] = normed.astype(bf16)


def merge(state, others, lam, gain, consts, vd):
    rows = state[1].shape[-1]
    vmem = pl.BlockSpec(memory_space=pltpu.VMEM)
    return pl.pallas_call(
        functools.partial(merge_body, consts, vd),
        out_shape=jax.ShapeDtypeStruct((rows, 2 * vd), bf16),
        in_specs=[vmem] * (4 + len(others)),
        out_specs=vmem,
        compiler_params=pltpu.CompilerParams(vmem_limit_bytes=12 * MIB),
        name="merge",
    )(lam.T, gain, *state, *others)


def project_body(n, share, *refs):
    at_ref, heads, outs = refs[0], refs[1 : 1 + n], refs[1 + n : 1 + 2 * n]
    residual_ref, gain_ref, normed_ref, cols_ref, summed_ref = refs[1 + 2 * n :]
    total = residual_ref[...].astype(f32)
    for h, o in zip(heads, outs):
        total = total + dot(h[...], o[...], 1, 0)
    summed_ref[...] = total
    inverse = lax.rsqrt(jnp.mean(total * total, axis=-1, keepdims=True) + eps_norm)
    normed_ref[...] = (summed_ref[...] * inverse * gain_ref[...]).astype(bf16)
    cols_ref[...] = summed_ref[:, pl.ds(pl.multiple_of(at_ref[0] * share, share), share)]


def project(at, heads, outs, residual, gain, share):
    n = len(heads)
    rows, wide = residual.shape
    vmem = pl.BlockSpec(memory_space=pltpu.VMEM)
    smem = pl.BlockSpec(memory_space=pltpu.SMEM)
    return pl.pallas_call(
        functools.partial(project_body, n, share),
        out_shape=(jax.ShapeDtypeStruct((rows, wide), bf16), jax.ShapeDtypeStruct((rows, share), f32)),
        in_specs=[smem] + [vmem] * (2 * n + 2),
        out_specs=(vmem, vmem),
        scratch_shapes=[pltpu.VMEM((rows, wide), f32)],
        compiler_params=pltpu.CompilerParams(vmem_limit_bytes=20 * MIB),
        cost_estimate=pl.CostEstimate(flops=2 * rows * wide * n * heads[0].shape[1], transcendentals=0, bytes_accessed=8 * MIB),
        name="project",
    )(at, *heads, *outs, residual, gain)


CUTS = 2


def hidden_body(at_ref, x_ref, w_ref, down_ref, hidden_ref, low_ref, high_ref, sum_ref):
    step = pl.program_id(0)
    spread, _, deep, units = w_ref.shape
    tall = spread * deep
    which, cut = step // CUTS, step % CUTS
    more = dot(x_ref[:, pl.ds(pl.multiple_of(cut * tall, tall), tall)], w_ref[...].reshape(tall, units), 1, 0)

    @pl.when(cut == 0)
    def _():
        sum_ref[which] = more

    @pl.when(cut > 0)
    def _():
        sum_ref[which] = sum_ref[which] + more

    @pl.when(step == 2 * CUTS - 1)
    def _():
        gate = sum_ref[0]
        hidden_ref[...] = (gate / (1.0 + jnp.exp(-gate)) * sum_ref[1]).astype(bf16)
        piece = dot(hidden_ref[...], down_ref[...].reshape(-1, units), 1, 1).astype(bf16)
        half = piece.shape[0] // 2
        low_ref[...] = piece[:half]
        high_ref[...] = piece[half:]


def hidden_of(at, x, w, n):
    rows, wide = x.shape
    spread, _, deep, units = w.shape
    share = wide // n
    whole = lambda p, at: (0, 0)
    return pl.pallas_call(
        hidden_body,
        grid_spec=pltpu.PrefetchScalarGridSpec(
            num_scalar_prefetch=1,
            grid=(2 * CUTS,),
            in_specs=[
                pl.BlockSpec((rows, wide), whole),
                pl.BlockSpec((spread // CUTS, 1, deep, units), lambda p, at: (p % CUTS, p // CUTS, 0, 0)),
                pl.BlockSpec((spread // n, 1, deep, units), lambda p, at: ((at[0] + 2) % n, 2, 0, 0)),
            ],
            out_specs=(
                pl.BlockSpec((rows, units), whole),
                pl.BlockSpec((rows // 2, share), whole),
                pl.BlockSpec((rows // 2, share), whole),
            ),
            scratch_shapes=[pltpu.VMEM((2, rows, units), f32)],
        ),
        out_shape=(
            jax.ShapeDtypeStruct((rows, units), bf16),
            jax.ShapeDtypeStruct((rows // 2, share), bf16),
            jax.ShapeDtypeStruct((rows // 2, share), bf16),
        ),
        compiler_params=pltpu.CompilerParams(vmem_limit_bytes=36 * MIB, dimension_semantics=("arbitrary",)),
        cost_estimate=pl.CostEstimate(flops=4 * rows * wide * units, transcendentals=rows * units, bytes_accessed=w.size * 2),
        name="hidden",
    )(at, x, w, w)


def own_body(at_ref, w_ref, hidden_ref, cols_ref, out_ref, buf, sem):
    part = buf.shape[0]
    copy = pltpu.make_async_copy(w_ref.at[pl.ds(at_ref[0] * part, part), 2], buf, sem)
    copy.start()
    copy.wait()
    out_ref[...] = cols_ref[...] + 0.5 * dot(hidden_ref[...], buf[...].reshape(-1, buf.shape[2]), 1, 1)


def own_part(at, hidden, w, cols, n):
    spread, _, deep, units = w.shape
    rows, share = cols.shape
    vmem = pl.BlockSpec(memory_space=pltpu.VMEM)
    return pl.pallas_call(
        own_body,
        out_shape=jax.ShapeDtypeStruct((rows, share), f32),
        in_specs=[pl.BlockSpec(memory_space=pltpu.SMEM), pl.BlockSpec(memory_space=pltpu.HBM), vmem, vmem],
        out_specs=vmem,
        scratch_shapes=[pltpu.VMEM((spread // n, deep, units), bf16), pltpu.SemaphoreType.DMA],
        compiler_params=pltpu.CompilerParams(vmem_limit_bytes=8 * MIB),
        cost_estimate=pl.CostEstimate(flops=2 * rows * share * units, transcendentals=0, bytes_accessed=2 * share * units),
        name="own",
    )(at, w, hidden, cols)


def sides_body(n, at_ref, w_ref, hidden_ref, low_ref, high_ref, up_ref, down_ref, buf, sem):
    part = buf.shape[1]
    half = low_ref.shape[0]
    copies = []
    for i, k in enumerate((1, n - 1)):
        j = (at_ref[0] + k) % n
        copies.append(pltpu.make_async_copy(w_ref.at[pl.ds(j * part, part), 2], buf.at[i], sem.at[i]))
        copies[i].start()
    copies[0].wait()
    piece = dot(hidden_ref[...], buf[0].reshape(-1, buf.shape[3]), 1, 1)
    up_ref[:half] = (piece[:half] + low_ref[...].astype(f32)).astype(bf16)
    up_ref[half:] = piece[half:].astype(bf16)
    copies[1].wait()
    piece = dot(hidden_ref[...], buf[1].reshape(-1, buf.shape[3]), 1, 1)
    down_ref[:half] = piece[:half].astype(bf16)
    down_ref[half:] = (piece[half:] + high_ref[...].astype(f32)).astype(bf16)


def side_parts(at, hidden, w, low, high, n):
    spread, _, deep, units = w.shape
    rows = hidden.shape[0]
    share = low.shape[1]
    vmem = pl.BlockSpec(memory_space=pltpu.VMEM)
    piece = jax.ShapeDtypeStruct((rows, share), bf16)
    return pl.pallas_call(
        functools.partial(sides_body, n),
        out_shape=(piece, piece),
        in_specs=[pl.BlockSpec(memory_space=pltpu.SMEM), pl.BlockSpec(memory_space=pltpu.HBM), vmem, vmem, vmem],
        out_specs=(vmem, vmem),
        scratch_shapes=[pltpu.VMEM((2, spread // n, deep, units), bf16), pltpu.SemaphoreType.DMA((2,))],
        compiler_params=pltpu.CompilerParams(vmem_limit_bytes=12 * MIB),
        cost_estimate=pl.CostEstimate(flops=4 * rows * share * units, transcendentals=0, bytes_accessed=4 * share * units),
        name="sides",
    )(at, w, hidden, low, high)


def local(
    residual,
    queries_a,
    keys_a,
    values_a,
    queries_b,
    keys_b,
    values_b,
    mix_lambda,
    head_gain,
    out_a,
    out_b,
    norm_gain,
    w_gate,
    w_up,
    w_down,
):
    wa = queries_a.shape[1] // 2
    wb = queries_b.shape[1] // 2
    vd = values_a.shape[1]
    consts = (wa**-0.5 * log2e, wb**-0.5 * log2e)
    n = lax.axis_size("tp")
    share = residual.shape[1] // n
    at = lax.axis_index("tp").astype(jnp.int32)[None]
    at, keys_a = lax.optimization_barrier((at, keys_a))

    kv, q = pack(((keys_a, keys_b, values_a, values_b), 1), ((queries_a, queries_b), 1))
    near = [kv, along_z(kv, 1), None, along_z(kv, 3)]
    queries = [q] + [along_y(q, k) for k in range(1, 4)]
    kv_far = other_core(kv)
    (oo,) = pack(((out_a, out_b), 0))
    outs = [oo] + [along_x(oo, k) for k in range(1, 4)]
    (three,) = pack(((w_gate, w_up, w_down.T), 0))
    three, queries[1], queries[3] = lax.optimization_barrier((three, queries[1], queries[3]))
    weights = lax.all_gather(three, "sp", axis=0, tiled=True)
    weights = in_hbm(weights.reshape(-1, 3, *w_gate.shape))
    kv, queries[1] = lax.optimization_barrier((kv, queries[1]))
    near[2] = along_z(kv, 2)

    go = functools.partial(attend, consts=consts, wa=wa, wb=wb, vd=vd)
    pairs = [[queries[k] for k in g] for g in ((2, 1), (3, 0))]
    state = go(pairs, [kv, kv_far], None, None)
    one, three, *state = lax.optimization_barrier((near[1], near[3], *state))
    far = {1: other_core(one), 3: other_core(three)}
    state = go(pairs, [one, three], state, None)
    two, *state = lax.optimization_barrier((near[2], *state))
    last = [far[1], far[3], two, other_core(two)]
    back = {}
    back[2], back[1] = go([[queries[2], queries[1]]], last, state, (0, 0, True))
    (back[3],) = go([[queries[3]]], last, state, (1, 0, True))
    back = {k: along_y(back[k], -k) for k in (2, 1, 3)}
    own = go([[queries[0]]], last, state, (1, 1, False))
    heads = merge(own, [back[k] for k in (1, 3, 2)], mix_lambda, head_gain, consts, vd)

    everyone = [heads] + [along_x(heads, k) for k in range(1, 4)]
    normed, cols = project(at, everyone, outs, residual, norm_gain[None], share)
    hidden, low, high = hidden_of(at, normed, weights, n)
    low, high = along_x(low, 1), along_x(high, -1)
    mine = own_part(at, hidden, weights, cols, n)
    up, down = side_parts(at, hidden, weights, low, high, n)
    arrived = along_x(up, 1).astype(f32) + along_x(down, -1).astype(f32)
    return (mine + 0.5 * arrived).astype(bf16)


def solution(mesh):
    in_specs = (
        P("sp", None),
        P("sp", "tp"),
        P("sp", "tp"),
        P("sp", "tp"),
        P("sp", "tp"),
        P("sp", "tp"),
        P("sp", "tp"),
        P(None, "tp"),
        P(),
        P("tp", None),
        P("tp", None),
        P(),
        P("sp", "tp"),
        P("sp", "tp"),
        P("tp", "sp"),
    )
    out_specs = P("sp", "tp")

    return jax.shard_map(local, mesh=mesh, in_specs=in_specs, out_specs=out_specs, check_vma=False)
```

```python
import math
import functools
import jax
import jax.numpy as jnp
from jax import lax
from jax.experimental import pallas as pl
from jax.experimental.pallas import tpu as pltpu
from jax.sharding import PartitionSpec as P

eps_norm = 1e-06
head_scale = 0.8
log2e = math.log2(math.e)
f32 = jnp.float32
bf16 = jnp.bfloat16

SP = [(z, y, c) for z in range(4) for y in range(4) for c in range(2)]


def place(z, y, c):
    return (z % 4) * 8 + (y % 4) * 2 + c % 2


def along_y(x, k):
    return lax.ppermute(x, "sp", [(place(z, y, c), place(z, y + k, c)) for z, y, c in SP])


def along_z(x, k):
    return lax.ppermute(x, "sp", [(place(z, y, c), place(z + k, y, c)) for z, y, c in SP])


def other_core(x):
    return lax.ppermute(x, "sp", [(place(z, y, c), place(z, y, c + 1)) for z, y, c in SP])


def along_x(x, k):
    return lax.ppermute(x, "tp", [(i, (i + k) % 4) for i in range(4)])


def dot(a, b, ca, cb):
    return lax.dot_general(a, b, (((ca,), (cb,)), ((), ())), preferred_element_type=f32)


def pack_body(layout, *refs):
    n = sum(len(parts) for parts in layout)
    ins, outs, sem = refs[:n], refs[n:-1], refs[-1]
    copies, i = [], 0
    for out, parts in zip(outs, layout):
        for corner in parts:
            part = tuple(pl.ds(c, d) for c, d in zip(corner, ins[i].shape))
            copies.append(pltpu.make_async_copy(ins[i], out.at[part], sem.at[i]))
            i += 1
    for c in copies:
        c.start()
    for c in copies:
        c.wait()


def in_hbm(x):
    return pltpu.with_memory_space_constraint(x, pltpu.HBM)


def pack(*sides, fixed=True):
    layout, shapes = [], []
    for arrays, axis in sides:
        at, corners = 0, []
        for a in arrays:
            corners.append((at, 0) if axis == 0 else (0, at))
            at += a.shape[axis]
        other = arrays[0].shape[1 - axis]
        layout.append(corners)
        shapes.append(jax.ShapeDtypeStruct((at, other) if axis == 0 else (other, at), arrays[0].dtype))
    flat = [in_hbm(a) if fixed else a for arrays, _ in sides for a in arrays]
    return pl.pallas_call(
        functools.partial(pack_body, layout),
        out_shape=tuple(shapes),
        in_specs=[pl.BlockSpec(memory_space=pltpu.HBM)] * len(flat),
        out_specs=tuple(pl.BlockSpec(memory_space=pltpu.VMEM) for _ in shapes),
        scratch_shapes=[pltpu.SemaphoreType.DMA((len(flat),))],
        compiler_params=pltpu.CompilerParams(vmem_limit_bytes=8 * MIB),
        name="pack",
    )(*flat)


PER = 2
AHEAD = 3
MIB = 1024 * 1024


def attend_body(groups, m, nk, carry, pick, consts, rows, wa, wb, vd, *refs):
    nq = groups * m
    q_refs, refs = refs[:nq], refs[nq:]
    kv_refs, refs = refs[:nk], refs[nk:]
    if carry:
        acc_in, ml_in, refs = refs[0], refs[1], refs[2:]
    send = pick is not None and pick[2]
    outs = m if send else 2
    q_buf, kv_buf, pad_buf, q_sem, kv_sem, acc_sem = refs[outs : outs + 6]
    turned = None
    rest = refs[outs + 6 :]
    if groups > 1:
        turned, rest = rest[0], rest[1:]
    if send:
        o_refs = refs[:m]
        acc_ref, ml_ref = rest
    else:
        acc_ref, ml_ref = refs[:2]
    q_copies = [
        pltpu.make_async_copy(q_refs[i], q_buf.at[i // m, pl.ds((i % m) * rows, rows)], q_sem.at[i]) for i in range(nq)
    ]
    kv_copies = [
        pltpu.make_async_copy(kv_refs[i], kv_buf.at[pl.ds(i * rows, rows)], kv_sem.at[i]) for i in range(nk)
    ]
    if carry:
        if pick is not None:
            lanes = pl.ds(pick[1] * rows, m * rows)
            acc_in = acc_in.at[pl.ds(pick[0], 1), :, lanes]
            ml_in = ml_in.at[pl.ds(pick[0], 1), :, lanes]
        acc_copies = [
            pltpu.make_async_copy(acc_in, acc_ref, acc_sem.at[0]),
            pltpu.make_async_copy(ml_in, ml_ref, acc_sem.at[1]),
        ]
    else:
        acc_copies = []
    per = min(PER, nk)
    for c in q_copies + kv_copies[:per] + acc_copies + kv_copies[per:]:
        c.start()
    if not carry:
        acc_ref[...] = jnp.zeros_like(acc_ref)
        ml_ref[:, 0:8, :] = jnp.full((groups, 8, m * rows), -jnp.inf, f32)
        ml_ref[:, 8:16, :] = jnp.zeros((groups, 8, m * rows), f32)
    for c in q_copies:
        c.wait()
    for g in range(groups):
        qa = q_buf[g, :, 0 : 2 * wa]
        col = lax.broadcasted_iota(jnp.int32, qa.shape, 1)
        zero = jnp.zeros_like(qa)
        pad_buf[g, :, 0 : 2 * wa] = jnp.where(col < wa, qa, zero)
        pad_buf[g, :, 2 * wa :] = jnp.where(col >= wa, qa, zero)
    for c in acc_copies:
        c.wait()
    steps = nk // per
    tall = per * rows
    wide = m * rows
    lane = 256 if wide % 256 == 0 else wide
    items = [(h, j) for h in range(wide // lane) for j in range(4)]

    def step(t, _):
        qi = t // steps
        ci = t % steps
        keys = pl.ds(pl.multiple_of(ci * tall, tall), tall)

        @pl.when(qi == 0)
        def _():
            for b in range(per):
                i = ci * per + b
                pltpu.make_async_copy(kv_refs[0], kv_buf.at[pl.ds(i * rows, rows)], kv_sem.at[i]).wait()
            if turned is not None:
                first = lax.broadcasted_iota(jnp.int32, (16, tall), 0) == 0
                for g in range(2):
                    at = 2 * wa + 2 * wb + g * vd
                    turned[ci, g, 0:vd, :] = kv_buf[keys, at : at + vd].T
                    turned[ci, g, vd : vd + 16, :] = jnp.where(first, 1.0, 0.0).astype(bf16)

        def score(h, j):
            lanes = slice(h * lane, (h + 1) * lane)
            if j < 2:
                return dot(kv_buf[keys, 0 : 2 * wa], pad_buf[qi, lanes, j * 2 * wa : (j + 1) * 2 * wa], 1, 1)
            at = 2 * wa + (j - 2) * wb
            return dot(kv_buf[keys, at : at + wb], q_buf[qi, lanes, at : at + wb], 1, 1)

        ready = [score(*item) for item in items[:AHEAD]]
        for n, (h, j) in enumerate(items):
            if n + AHEAD < len(items):
                ready.append(score(*items[n + AHEAD]))
            s = ready.pop(0)
            lanes = slice(h * lane, (h + 1) * lane)
            c = consts[j // 2]
            old = ml_ref[qi, j : j + 1, lanes]
            top = jnp.maximum(old, jnp.max(s, axis=0, keepdims=True))
            w = jnp.exp2((s - top) * c)
            decay = jnp.exp2((old - top) * c)
            ml_ref[qi, j : j + 1, lanes] = top
            if turned is not None:
                more = dot(turned[ci, j // 2], w.astype(bf16), 1, 0)
                total = more[vd : vd + 1]
                more = more[0:vd]
            else:
                total = jnp.sum(w, axis=0, keepdims=True)
                at = 2 * wa + 2 * wb + (j // 2) * vd
                more = dot(kv_buf[keys, at : at + vd], w.astype(bf16), 0, 0)
            ml_ref[qi, j + 8 : j + 9, lanes] = ml_ref[qi, j + 8 : j + 9, lanes] * decay + total
            part = slice(j * vd, (j + 1) * vd)
            acc_ref[qi, part, lanes] = acc_ref[qi, part, lanes] * decay + more
        return 0

    lax.fori_loop(0, groups * steps, step, 0)
    if send:
        level = level_of(ml_ref, consts)
        high = level.astype(bf16).astype(f32)
        mid = (level - high).astype(bf16).astype(f32)
        low = level - high - mid
        stats = jnp.concatenate([high, mid, low, jnp.zeros_like(low)], axis=0).astype(bf16)
        for i, o_ref in enumerate(o_refs):
            lanes = slice(i * rows, (i + 1) * rows)
            for j in range(4):
                part = slice(j * vd, (j + 1) * vd)
                inverse = 1.0 / ml_ref[0, j + 8 : j + 9, lanes]
                o_ref[part, :] = (acc_ref[0, part, lanes] * inverse).astype(bf16)
            o_ref[4 * vd :, :] = stats[:, lanes]


def level_of(ml_ref, consts):
    row = lax.broadcasted_iota(jnp.int32, (8, ml_ref.shape[2]), 0)
    used = row < 4
    top = jnp.where(used, ml_ref[0, 0:8, :], 0.0)
    total = jnp.where(used, ml_ref[0, 8:16, :], 1.0)
    return top * jnp.where(row < 2, consts[0], consts[1]) + jnp.log2(total)


def attend(queries, blocks, state, pick, consts, wa, wb, vd):
    groups, m = len(queries), len(queries[0])
    flat = [q for g in queries for q in g]
    nq, nk = len(flat), len(blocks)
    rows = flat[0].shape[0]
    wide = flat[0].shape[1]
    cols = blocks[0].shape[1]
    anywhere = pl.BlockSpec(memory_space=pl.ANY)
    vmem = pl.BlockSpec(memory_space=pltpu.VMEM)
    acc_shape = (groups, 4 * vd, m * rows)
    ml_shape = (groups, 16, m * rows)
    scratch = [
        pltpu.VMEM((groups, m * rows, wide), bf16),
        pltpu.VMEM((nk * rows, cols), bf16),
        pltpu.VMEM((groups, m * rows, 4 * wa), bf16),
        pltpu.SemaphoreType.DMA((nq,)),
        pltpu.SemaphoreType.DMA((nk,)),
        pltpu.SemaphoreType.DMA((2,)),
    ]
    if groups > 1:
        per = min(PER, nk)
        scratch.append(pltpu.VMEM((nk // per, 2, vd + 16, per * rows), bf16))
    if pick is not None and pick[2]:
        out_shape = (jax.ShapeDtypeStruct((4 * vd + 32, rows), bf16),) * m
        out_specs = (vmem,) * m
        scratch += [pltpu.VMEM(acc_shape, f32), pltpu.VMEM(ml_shape, f32)]
    else:
        out_shape = (jax.ShapeDtypeStruct(acc_shape, f32), jax.ShapeDtypeStruct(ml_shape, f32))
        out_specs = (vmem, vmem)
    work = nq * nk * rows * rows
    return pl.pallas_call(
        functools.partial(attend_body, groups, m, nk, state is not None, pick, consts, rows, wa, wb, vd),
        out_shape=out_shape,
        in_specs=[anywhere] * (nq + nk + (0 if state is None else 2)),
        out_specs=out_specs,
        scratch_shapes=scratch,
        compiler_params=pltpu.CompilerParams(vmem_limit_bytes=16 * MIB),
        cost_estimate=pl.CostEstimate(flops=work * 4 * 4 * vd, transcendentals=4 * work, bytes_accessed=nk * rows * cols * 2),
        name="attend",
    )(*flat, *blocks, *(state or ()))


def merge_body(consts, vd, lam_ref, gain_ref, acc_ref, ml_ref, *refs):
    others, out_ref = refs[:-1], refs[-1]
    levels = [level_of(ml_ref, consts)]
    for o in others:
        stats = o[4 * vd :, :].astype(f32)
        levels.append(stats[0:8] + stats[8:16] + stats[16:24])
    top = functools.reduce(jnp.maximum, levels)
    shares = [jnp.exp2(v - top) for v in levels]
    inverse = 1.0 / functools.reduce(jnp.add, shares)
    shares = [v * inverse for v in shares]
    for g in range(2):
        ratio = []
        for j in (2 * g, 2 * g + 1):
            part = slice(j * vd, (j + 1) * vd)
            value = acc_ref[0, part, :] * (shares[0][j : j + 1] / ml_ref[0, j + 8 : j + 9, :])
            for o, share in zip(others, shares[1:]):
                value = value + o[part, :].astype(f32) * share[j : j + 1]
            ratio.append(value)
        mixed = ratio[0] - lam_ref[0:1, g : g + 1] * ratio[1]
        scale = lax.rsqrt(jnp.mean(mixed * mixed, axis=0, keepdims=True) + eps_norm)
        normed = (mixed * scale).T * gain_ref[g : g + 1, :] * head_scale
        out_ref[:, g * vd : (g + 1) * vd] = normed.astype(bf16)


def merge(state, others, lam, gain, consts, vd):
    rows = state[1].shape[-1]
    vmem = pl.BlockSpec(memory_space=pltpu.VMEM)
    return pl.pallas_call(
        functools.partial(merge_body, consts, vd),
        out_shape=jax.ShapeDtypeStruct((rows, 2 * vd), bf16),
        in_specs=[vmem] * (4 + len(others)),
        out_specs=vmem,
        compiler_params=pltpu.CompilerParams(vmem_limit_bytes=12 * MIB),
        name="merge",
    )(lam.T, gain, *state, *others)


def project_body(n, share, *refs):
    at_ref, heads, outs = refs[0], refs[1 : 1 + n], refs[1 + n : 1 + 2 * n]
    residual_ref, gain_ref, normed_ref, cols_ref, summed_ref = refs[1 + 2 * n :]
    total = residual_ref[...].astype(f32)
    for h, o in zip(heads, outs):
        total = total + dot(h[...], o[...], 1, 0)
    summed_ref[...] = total
    inverse = lax.rsqrt(jnp.mean(total * total, axis=-1, keepdims=True) + eps_norm)
    normed_ref[...] = (summed_ref[...] * inverse * gain_ref[...]).astype(bf16)
    cols_ref[...] = summed_ref[:, pl.ds(pl.multiple_of(at_ref[0] * share, share), share)]


def project(at, heads, outs, residual, gain, share):
    n = len(heads)
    rows, wide = residual.shape
    vmem = pl.BlockSpec(memory_space=pltpu.VMEM)
    smem = pl.BlockSpec(memory_space=pltpu.SMEM)
    return pl.pallas_call(
        functools.partial(project_body, n, share),
        out_shape=(jax.ShapeDtypeStruct((rows, wide), bf16), jax.ShapeDtypeStruct((rows, share), f32)),
        in_specs=[smem] + [vmem] * (2 * n + 2),
        out_specs=(vmem, vmem),
        scratch_shapes=[pltpu.VMEM((rows, wide), f32)],
        compiler_params=pltpu.CompilerParams(vmem_limit_bytes=20 * MIB),
        cost_estimate=pl.CostEstimate(flops=2 * rows * wide * n * heads[0].shape[1], transcendentals=0, bytes_accessed=8 * MIB),
        name="project",
    )(at, *heads, *outs, residual, gain)


def assemble_body(n, place_ref, *refs):
    firsts, seconds, outs = refs[: 2 * n], refs[2 * n : 4 * n], refs[4 * n : 4 * n + 3]
    sem = refs[4 * n + 3]
    deep = outs[0].shape[1]
    spot = place_ref[1]
    y_here, z_here, core_here = (spot // 2) % 4, spot // 8, spot % 2
    for c in range(2):
        core = (core_here + c) % 2
        for i in range(n):

            def one(r, _):
                to = ((z_here + 4 - i) % 4) * 8 + ((y_here + 4 - r) % 4) * 2 + core
                first = firsts[c * n + i]
                pltpu.make_async_copy(first.at[r, pl.ds(0, deep)], outs[0].at[to], sem.at[0]).start()
                pltpu.make_async_copy(first.at[r, pl.ds(deep, deep)], outs[2].at[to], sem.at[2]).start()
                to = ((z_here + 4 - r) % 4) * 8 + ((y_here + 4 - i) % 4) * 2 + core
                pltpu.make_async_copy(seconds[c * n + i].at[r], outs[1].at[to], sem.at[1]).start()
                return 0

            lax.fori_loop(0, 4, one, 0)
    for i in range(3):
        pltpu.make_async_copy(outs[i], outs[i], sem.at[i]).wait()


def assemble(place, firsts, seconds, n):
    _, deep, units = seconds[0].shape
    shape = jax.ShapeDtypeStruct((8 * n, deep, units), bf16)
    vmem = pl.BlockSpec(memory_space=pltpu.VMEM)
    return pl.pallas_call(
        functools.partial(assemble_body, n),
        out_shape=(shape,) * 3,
        in_specs=[pl.BlockSpec(memory_space=pltpu.SMEM)] + [pl.BlockSpec(memory_space=pl.ANY)] * (4 * n),
        out_specs=(vmem,) * 3,
        scratch_shapes=[pltpu.SemaphoreType.DMA((3,))],
        compiler_params=pltpu.CompilerParams(vmem_limit_bytes=20 * MIB),
        name="assemble",
    )(place, *firsts, *seconds)


def product(hidden, down_ref, j, n):
    part = down_ref.shape[0] // n
    w = down_ref[pl.ds(j * part, part)].reshape(part * down_ref.shape[1], down_ref.shape[2])
    return dot(hidden, w, 1, 1)


LANES = 256


def hidden_body(n, place_ref, x_ref, gate_ref, up_ref, down_ref, hidden_ref, low_ref, high_ref):
    spread, deep, units = gate_ref.shape
    full = units // LANES

    def some(lanes, width):
        gate = dot(x_ref[...], gate_ref[:, :, lanes].reshape(spread * deep, width), 1, 0)
        up = dot(x_ref[...], up_ref[:, :, lanes].reshape(spread * deep, width), 1, 0)
        hidden_ref[:, lanes] = (gate / (1.0 + jnp.exp(-gate)) * up).astype(bf16)

    def one(i, _):
        some(pl.ds(pl.multiple_of(i * LANES, LANES), LANES), LANES)
        return 0

    lax.fori_loop(0, full, one, 0)
    if units % LANES:
        some(slice(full * LANES, units), units % LANES)
    piece = product(hidden_ref[...], down_ref, (place_ref[0] + 2) % n, n).astype(bf16)
    half = piece.shape[0] // 2
    low_ref[...] = piece[:half]
    high_ref[...] = piece[half:]


def hidden_of(place, x, gate, up, down, n):
    rows, wide = x.shape
    units = gate.shape[-1]
    vmem = pl.BlockSpec(memory_space=pltpu.VMEM)
    half = jax.ShapeDtypeStruct((rows // 2, wide // n), bf16)
    return pl.pallas_call(
        functools.partial(hidden_body, n),
        out_shape=(jax.ShapeDtypeStruct((rows, units), bf16), half, half),
        in_specs=[pl.BlockSpec(memory_space=pltpu.SMEM)] + [vmem] * 4,
        out_specs=(vmem,) * 3,
        compiler_params=pltpu.CompilerParams(vmem_limit_bytes=26 * MIB),
        cost_estimate=pl.CostEstimate(flops=4 * rows * wide * units, transcendentals=rows * units, bytes_accessed=gate.size * 4),
        name="hidden",
    )(place, x, gate, up, down)


def own_body(n, place_ref, hidden_ref, down_ref, cols_ref, out_ref):
    out_ref[...] = cols_ref[...] + 0.5 * product(hidden_ref[...], down_ref, place_ref[0], n)


def own_part(place, hidden, down, cols, n):
    rows, share = cols.shape
    units = hidden.shape[1]
    vmem = pl.BlockSpec(memory_space=pltpu.VMEM)
    return pl.pallas_call(
        functools.partial(own_body, n),
        out_shape=jax.ShapeDtypeStruct((rows, share), f32),
        in_specs=[pl.BlockSpec(memory_space=pltpu.SMEM)] + [vmem] * 3,
        out_specs=vmem,
        compiler_params=pltpu.CompilerParams(vmem_limit_bytes=14 * MIB),
        cost_estimate=pl.CostEstimate(flops=2 * rows * share * units, transcendentals=0, bytes_accessed=2 * share * units),
        name="own",
    )(place, hidden, down, cols)


def sides_body(n, place_ref, hidden_ref, down_ref, low_ref, high_ref, next_ref, prev_ref):
    half = low_ref.shape[0]
    piece = product(hidden_ref[...], down_ref, (place_ref[0] + 1) % n, n)
    next_ref[:half] = (piece[:half] + low_ref[...].astype(f32)).astype(bf16)
    next_ref[half:] = piece[half:].astype(bf16)
    piece = product(hidden_ref[...], down_ref, (place_ref[0] + n - 1) % n, n)
    prev_ref[:half] = piece[:half].astype(bf16)
    prev_ref[half:] = (piece[half:] + high_ref[...].astype(f32)).astype(bf16)


def side_parts(place, hidden, down, low, high, n):
    rows, units = hidden.shape
    share = low.shape[1]
    vmem = pl.BlockSpec(memory_space=pltpu.VMEM)
    piece = jax.ShapeDtypeStruct((rows, share), bf16)
    return pl.pallas_call(
        functools.partial(sides_body, n),
        out_shape=(piece, piece),
        in_specs=[pl.BlockSpec(memory_space=pltpu.SMEM)] + [vmem] * 4,
        out_specs=(vmem, vmem),
        compiler_params=pltpu.CompilerParams(vmem_limit_bytes=16 * MIB),
        cost_estimate=pl.CostEstimate(flops=4 * rows * share * units, transcendentals=0, bytes_accessed=4 * share * units),
        name="sides",
    )(place, hidden, down, low, high)


def local(
    residual,
    queries_a,
    keys_a,
    values_a,
    queries_b,
    keys_b,
    values_b,
    mix_lambda,
    head_gain,
    out_a,
    out_b,
    norm_gain,
    w_gate,
    w_up,
    w_down,
):
    wa = queries_a.shape[1] // 2
    wb = queries_b.shape[1] // 2
    vd = values_a.shape[1]
    consts = (wa**-0.5 * log2e, wb**-0.5 * log2e)
    n = lax.axis_size("tp")
    share = residual.shape[1] // n
    where = jnp.stack([lax.axis_index("tp"), lax.axis_index("sp")]).astype(jnp.int32)
    where, keys_a = lax.optimization_barrier((where, keys_a))
    deep, units = w_gate.shape

    kv, q = pack(((keys_a, keys_b, values_a, values_b), 1), ((queries_a, queries_b), 1))
    near = [kv, along_z(kv, 1), None, along_z(kv, 3)]
    queries = [q] + [along_y(q, k) for k in (1, 2, 3)]
    first, second = pack(((w_gate, w_down.T), 0), ((w_up,), 0))
    firsts = [first] + [along_y(first, k) for k in (1, 2, 3)]
    seconds = [second] + [along_z(second, k) for k in (1, 2, 3)]
    kv_far = other_core(kv)
    near[2] = along_z(kv, 2)
    (oo,) = pack(((out_a, out_b), 0))
    outs = [oo] + [along_x(oo, k) for k in (1, 2, 3)]
    first, second = pack((firsts, 0), (seconds, 0), fixed=False)
    firsts = [first] + [along_z(first, k) for k in (1, 2, 3)]
    seconds = [second] + [along_y(second, k) for k in (1, 2, 3)]

    go = functools.partial(attend, consts=consts, wa=wa, wb=wb, vd=vd)
    pairs = [[queries[k] for k in g] for g in ((2, 1), (3, 0))]
    state = go(pairs, [kv, kv_far], None, None)
    one, three, *state = lax.optimization_barrier((near[1], near[3], *state))
    far = {1: other_core(one), 3: other_core(three)}
    state = go(pairs, [one, three], state, None)
    two, *state = lax.optimization_barrier((near[2], *state))
    last = [far[1], far[3], two, other_core(two)]
    back = {}
    back[2], back[1] = go([[queries[2], queries[1]]], last, state, (0, 0, True))
    (back[3],) = go([[queries[3]]], last, state, (1, 0, True))
    back = {k: along_y(back[k], -k) for k in (2, 1, 3)}
    own = list(go([[queries[0]]], last, state, (1, 1, False)))
    late = firsts[2]
    *mid, own[1] = lax.optimization_barrier((firsts[0], firsts[1], firsts[3], *seconds, own[1]))
    seconds = mid[3:] + [other_core(a) for a in mid[3:]]
    others = [other_core(a) for a in mid[:3]]
    heads = merge(own, [back[k] for k in (1, 3, 2)], mix_lambda, head_gain, consts, vd)

    heads, late = lax.optimization_barrier((heads, late))
    everyone = [heads] + [along_x(heads, k) for k in (1, 2, 3)]
    firsts = [mid[0], mid[1], late, mid[2], others[0], others[1], other_core(late), others[2]]
    firsts = [a.reshape(4, 2 * deep, units) for a in firsts]
    seconds = [a.reshape(4, deep, units) for a in seconds]
    gate, up, down = assemble(where, firsts, seconds, n)
    normed, cols = project(where, everyone, outs, residual, norm_gain[None], share)
    hidden, low, high = hidden_of(where, normed, gate, up, down, n)
    low, high = along_x(low, 1), along_x(high, -1)
    mine = own_part(where, hidden, down, cols, n)
    ahead, behind = side_parts(where, hidden, down, low, high, n)
    arrived = along_x(ahead, 1).astype(f32) + along_x(behind, -1).astype(f32)
    return (mine + 0.5 * arrived).astype(bf16)


def solution(mesh):
    in_specs = (
        P("sp", None),
        P("sp", "tp"),
        P("sp", "tp"),
        P("sp", "tp"),
        P("sp", "tp"),
        P("sp", "tp"),
        P("sp", "tp"),
        P(None, "tp"),
        P(),
        P("tp", None),
        P("tp", None),
        P(),
        P("sp", "tp"),
        P("sp", "tp"),
        P("tp", "sp"),
    )
    out_specs = P("sp", "tp")

    return jax.shard_map(local, mesh=mesh, in_specs=in_specs, out_specs=out_specs, check_vma=False)
```
